256 devices in a mesh: sp: 64 (over z, x, core), tp: 4 (over y).
Axes of the slice: x: 4, y: 4, z: 8, core: 2. Of those that a mesh axis runs over, the one named last changes fastest.
Arguments:
- tokens: bfloat16 [16384, 2048], P('sp', 'tp'), may hold values from -6 to 6
- norm_gain: float32 [2048], replicated, may hold values from 0.1 to 1.9
- query_one: bfloat16 [2048, 512], P('sp', 'tp'), may hold values from -1 to 1
- key_one: bfloat16 [2048, 512], P('sp', 'tp'), may hold values from -1 to 1
- query_two: bfloat16 [2048, 512], P('sp', 'tp'), may hold values from -0.15625 to 0.15625
- key_two: bfloat16 [2048, 512], P('sp', 'tp'), may hold values from -0.15625 to 0.15625
- value_weight: bfloat16 [2048, 1024], P('sp', 'tp'), may hold values from -0.5 to 0.5
- pool_weight: bfloat16 [2048, 1024], P('sp', 'tp'), may hold values from -0.125 to 0.125
- lambda_head: float32 [8], replicated, may hold values from 0.3 to 0.8
- head_gain: float32 [128], replicated, may hold values from 0.1 to 1.9
- group_weight: bfloat16 [8, 128, 128], replicated, may hold values from -0.5 to 0.5
- pool_scale: float32 [1024], replicated, may hold values from 0.1 to 1.9
- out_attn: bfloat16 [1024, 2048], P('tp', 'sp'), may hold values from -0.125 to 0.125
- out_pool: bfloat16 [1024, 2048], P('tp', 'sp'), may hold values from -0.125 to 0.125
Outputs:
- mixed: bfloat16 [16384, 2048], P(('sp', 'tp'))
The draws below stay inside these ranges and needn't reach their ends.
All inputs are finite; a program needn't handle non-finite values.
Results may differ from the reference program's by a relative error of at most 0.013.
Values may be sent and summed in bfloat16 or wider, within the bound.
A program may use at most 128 MiB of HBM per device.

```python
import math
import jax
import jax.numpy as jnp
from jax import lax

D = 2048
HEADS = 8
HEAD_DIM = 64
VALUE_DIM = 128
GROUPS = 8
GROUP_DIM = 128
TOKENS = 16384


def paired_weights(key):
    first_draw = jax.random.normal(jax.random.fold_in(key, 101), (D, HEADS * HEAD_DIM), jnp.float32)
    second_draw = jax.random.normal(jax.random.fold_in(key, 202), (D, HEADS * HEAD_DIM), jnp.float32)
    query_part = jnp.clip(first_draw, -4.0, 4.0) * (1.3 / jnp.sqrt(jnp.float32(D)))
    key_part = jnp.clip(second_draw, -4.0, 4.0) * (1.3 / jnp.sqrt(jnp.float32(D)))
    return (query_part, key_part)


def draw_query_one(key, part):
    return paired_weights(key)[0].astype(jnp.bfloat16)


def draw_key_one(key, part):
    return paired_weights(key)[1].astype(jnp.bfloat16)


def levels(rng, shape, shards, smallest, high):
    gain = 1.0
    for position, blocks in shards:
        steps = jax.random.uniform(jax.random.fold_in(jax.random.fold_in(rng, 6), position), (blocks,), jnp.float32, smallest / len(shards), high / len(shards))
        gain = gain * jnp.repeat(jnp.exp(steps), shape[position] // blocks).reshape((-1,) + (1,) * (len(shape) - 1 - position))
    return gain


def normal_values(key, extent, spread, limit, split=(), held_as=jnp.bfloat16):
    loudness = levels(key, extent, split, -0.22, 0.18) if split else 1.0
    array = jax.random.normal(key, extent, jnp.float32) * spread * loudness
    return jnp.minimum(jnp.maximum(array, -limit), limit).astype(held_as)


def setup_inputs(seed: int = 0) -> dict:
    arg_keys = jax.random.split(jax.random.key(seed), 15)
    return {
        "tokens": normal_values(arg_keys[0], (TOKENS, D), 1.0, 6.0, ((0, 64), (1, 4))),
        "norm_gain": jnp.clip(1.0 + 0.18 * jax.random.normal(arg_keys[1], (D,), jnp.float32), 0.1, 1.9),
        "query_one": draw_query_one(jax.random.fold_in(arg_keys[14], 71), 0),
        "key_one": draw_key_one(jax.random.fold_in(arg_keys[14], 71), 0),
        "query_two": normal_values(arg_keys[4], (D, HEADS * HEAD_DIM), (D * 100 // 169) ** -0.5, 0.15625, ((0, 64), (1, 4))),
        "key_two": normal_values(arg_keys[5], (D, HEADS * HEAD_DIM), (D * 100 // 169) ** -0.5, 0.15625, ((0, 64), (1, 4))),
        "value_weight": normal_values(arg_keys[6], (D, HEADS * VALUE_DIM), (D // 16) ** -0.5, 0.5, ((0, 64), (1, 4))),
        "pool_weight": normal_values(arg_keys[7], (D, GROUPS * GROUP_DIM), D ** -0.5, 0.125, ((0, 64), (1, 4))),
        "lambda_head": jnp.clip(jax.random.uniform(arg_keys[8], (HEADS,), jnp.float32, 0.3, 0.8), 0.3, 0.8),
        "head_gain": jnp.clip(1.0 + 0.18 * jax.random.normal(arg_keys[9], (VALUE_DIM,), jnp.float32), 0.1, 1.9),
        "group_weight": normal_values(arg_keys[10], (GROUPS, GROUP_DIM, GROUP_DIM), GROUP_DIM ** -0.5, 0.5),
        "pool_scale": jnp.clip(1.0 + 0.18 * jax.random.normal(arg_keys[11], (GROUPS * GROUP_DIM,), jnp.float32), 0.1, 1.9),
        "out_attn": normal_values(arg_keys[12], (HEADS * VALUE_DIM, D), (HEADS * VALUE_DIM + GROUPS * GROUP_DIM) ** -0.5, 0.125, ((0, 4), (1, 64))),
        "out_pool": normal_values(arg_keys[13], (GROUPS * GROUP_DIM, D), (HEADS * VALUE_DIM + GROUPS * GROUP_DIM) ** -0.5, 0.125, ((0, 4), (1, 64))),
    }


rope_base = 500000.0
head_scale = 0.8
norm_floor = 1e-06
head_floor = 0.001
masked_score = -1e+30

def rotate(values_in, positions):
    half_dim = values_in.shape[-1] // 2
    inverse = rope_base ** (-(jnp.arange(half_dim, dtype=jnp.float32) * 2.0 / values_in.shape[-1]))
    angles = positions.astype(jnp.float32)[:, None] * inverse[None, :]
    cosine = jnp.cos(angles)[:, None, :]
    sine_part = jnp.sin(angles)[:, None, :]
    first_half = values_in[..., :half_dim]
    second_half = values_in[..., half_dim:]
    return jnp.concatenate([first_half * cosine - second_half * sine_part, second_half * cosine + first_half * sine_part], axis=-1)

def reference(tokens, norm_gain, query_one, key_one, query_two, key_two, value_weight, pool_weight, lambda_head, head_gain, group_weight, pool_scale, out_attn, out_pool):
    float_rows = tokens.astype(jnp.float32)
    normed = (float_rows * lax.rsqrt(lax.optimization_barrier(jnp.mean(float_rows * float_rows, axis=-1, keepdims=True)) + norm_floor) * norm_gain).astype(jnp.bfloat16)
    positions = jnp.arange(TOKENS, dtype=jnp.int32)
    score_scale = HEAD_DIM ** (-0.5)

    def project(weight):
        return jnp.dot(normed, weight, preferred_element_type=jnp.float32)

    def turned(weight):
        rounded_rows = rotate(project(weight).reshape(TOKENS, HEADS, HEAD_DIM), positions).astype(jnp.bfloat16)
        return lax.optimization_barrier(rounded_rows).astype(jnp.float32)
    query_a = turned(query_one)
    key_a = turned(key_one)
    query_b = turned(query_two)
    key_b = turned(key_two)
    value_rows = lax.optimization_barrier(project(value_weight).astype(jnp.bfloat16)).astype(jnp.float32).reshape(TOKENS, HEADS, VALUE_DIM)
    query_block = math.gcd(TOKENS, 256)
    blocks = TOKENS // query_block

    def one_block(block_id):
        start_row = block_id * query_block
        query_pos = start_row + jnp.arange(query_block, dtype=jnp.int32)
        visible = (positions[None, :] <= query_pos[:, None])[:, None, :]
        map_means = []
        for query_all, key_all in ((query_a, key_a), (query_b, key_b)):
            query_part = lax.dynamic_slice_in_dim(query_all, start_row, query_block, 0)
            scores = jnp.einsum('qhd,khd->qhk', query_part, key_all) * score_scale
            scores = jnp.where(visible, scores, masked_score)
            top_row = lax.optimization_barrier(jnp.max(scores, axis=-1, keepdims=True))
            weights = jnp.where(visible, jnp.exp(scores - top_row), 0.0)
            totals = lax.optimization_barrier(jnp.sum(weights, axis=-1))
            rounded = lax.optimization_barrier(weights.astype(jnp.bfloat16)).astype(jnp.float32)
            map_means.append(jnp.einsum('qhk,khd->qhd', rounded, value_rows) / totals[..., None])
        differed = map_means[0] - lambda_head[None, :, None] * map_means[1]
        scaled = differed * lax.rsqrt(lax.optimization_barrier(jnp.mean(differed * differed, axis=-1, keepdims=True)) + head_floor) * head_gain * head_scale
        return scaled.astype(jnp.bfloat16)
    attn_out = lax.map(one_block, jnp.arange(blocks, dtype=jnp.int32)).reshape(TOKENS, HEADS * VALUE_DIM)
    pool_rows = lax.optimization_barrier(project(pool_weight).astype(jnp.bfloat16)).astype(jnp.float32)
    running = jnp.cumsum(pool_rows, axis=0)
    results = []
    for group_id in range(GROUPS):
        window = 2 ** (group_id % 4 + 1)
        first_col = group_id * GROUP_DIM
        section = running[:, first_col:first_col + GROUP_DIM]
        earlier = jnp.pad(section, ((window, 0), (0, 0)))[:TOKENS]
        counts = jnp.minimum(positions + 1, window).astype(jnp.float32)
        window_mean = (section - earlier) / counts[:, None] - pool_rows[:, first_col:first_col + GROUP_DIM]
        results.append(jnp.dot(window_mean.astype(jnp.bfloat16), group_weight[group_id], preferred_element_type=jnp.float32))
    pooled = (jnp.concatenate(results, axis=1) * pool_scale).astype(jnp.bfloat16)
    mixed = jnp.dot(attn_out, out_attn, preferred_element_type=jnp.float32) + jnp.dot(pooled, out_pool, preferred_element_type=jnp.float32)
    return mixed.astype(jnp.bfloat16)
```

```python
import math

import jax
import jax.numpy as jnp
import numpy as np
from jax import lax
from jax.experimental import pallas as pl
from jax.experimental.pallas import tpu as pltpu
from jax.sharding import PartitionSpec as P

MESH = pl.DeviceIdType.MESH
F32 = jnp.float32
BF16 = jnp.bfloat16
Z_SIZE = 8
X_SIZE = 4
LANE_TILE = 256

rope_base = 500000.0
head_scale = 0.8
norm_floor = 1e-06
head_floor = 0.001
low_score = -1e30


def rope_tables(chip_tokens, chips):
    lane = np.arange(128)
    inverse = rope_base ** (-((lane % 32) * 2.0 / 64.0))
    sign = np.where(lane % 64 < 32, -1.0, 1.0)
    near = np.arange(chip_tokens)[:, None] * inverse[None, :]
    far = (np.arange(chips) * chip_tokens)[:, None] * inverse[None, :]
    return (
        np.cos(near).astype(np.float32),
        (np.sin(near) * sign).astype(np.float32),
        np.cos(far).astype(np.float32),
        (np.sin(far) * sign).astype(np.float32),
    )


class Ring:
    def __init__(self, n, me, device, unit, sems):
        self.n, self.me, self.device, self.unit = n, me, device, unit
        self.sems = {}
        for h in range(1, n // 2 + 1):
            for d in (0, 1):
                for u in (0, 1):
                    if self.has(d, h, u):
                        self.sems[d, h, u] = sems()

    def has(self, d, h, u):
        return h < self.n // 2 or (h == self.n // 2 and d == u)

    def slot(self, d, h):
        sign = 1 if d == 0 else -1
        return lax.rem(self.me - sign * h + self.n, self.n)

    def copy(self, d, h, u, slot):
        ref = self.unit(u, slot)
        send_sem, recv_sem = self.sems[d, h, u]
        return pltpu.make_async_remote_copy(
            src_ref=ref,
            dst_ref=ref,
            send_sem=send_sem,
            recv_sem=recv_sem,
            device_id=self.device(1 if d == 0 else -1),
            device_id_type=MESH,
        )

    def send(self, d, h, u):
        self.copy(d, h, u, self.slot(d, h - 1)).start()

    def begin(self, units=(0, 1)):
        for u in units:
            for d in (0, 1):
                if self.has(d, 1, u):
                    self.send(d, 1, u)

    def step(self, h):
        for u in (0, 1):
            for d in (0, 1):
                if self.has(d, h, u):
                    self.copy(d, h, u, self.slot(d, h)).wait_recv()
                    if (d, h + 1, u) in self.sems:
                        self.send(d, h + 1, u)

    def finish(self):
        for d, h, u in self.sems:
            self.copy(d, h, u, self.slot(d, h - 1)).wait_send()


def dot(a, b, dims=((1,), (0,))):
    return lax.dot_general(a, b, (dims, ((), ())), preferred_element_type=F32)


def make_kernel(zs, xs, ys, tok, wide):
    chip = 2 * tok
    kz = wide // zs
    part = wide // ys
    kb = min(kz, part)
    quarter = tok // ys
    tiles = 2 * chip // LANE_TILE

    def kernel(
        tokens, gain, q1, k1, q2, k2, vw, pw, lam, hgain, gw, pscale, oa, op,
        cos_near, sin_near, cos_far, sin_far,
        out,
        wsend, wbuf, wt, tokbuf, nrm, proj, kbuf, vbuf, qz, acc, mbuf, lbuf,
        pext, halo_x, halo_z, o1s, e1s, o1r, e1r, o2s, e2s, o2r, e2r, abuf,
        ysum, y1r, y2s, y2r, send_sems, recv_sems,
    ):
        sp = lax.axis_index("sp")
        y = lax.axis_index("tp")
        core = lax.rem(sp, 2)
        place = sp // 2
        x = lax.rem(place, xs)
        z = place // xs
        other = 1 - core
        head = 2 * y + core

        def at_z(step):
            return {"sp": (lax.rem(z + step + zs, zs) * xs + x) * 2 + core, "tp": y}

        def at_x(step):
            return {"sp": (z * xs + lax.rem(x + step + xs, xs)) * 2 + core, "tp": y}

        def at_y(step):
            return {"sp": sp, "tp": lax.rem(y + step + ys, ys)}

        def at_partner():
            return {"sp": place * 2 + other, "tp": y}

        used = [0]

        def sems():
            k = used[0]
            used[0] += 1
            return send_sems.at[k], recv_sems.at[k]

        def remote(src, dst, device):
            send_sem, recv_sem = sems()
            return pltpu.make_async_remote_copy(
                src_ref=src, dst_ref=dst, send_sem=send_sem, recv_sem=recv_sem,
                device_id=device, device_id_type=MESH,
            )

        sent = []

        def post(copy):
            copy.start()
            sent.append(copy)
            return copy

        def by_head(h):
            a, b = h * 64, h * 64 + 64
            c, d = h * 128, h * 128 + 128
            return jnp.concatenate(
                [q1[:, a:b], q2[:, a:b], k1[:, a:b], k2[:, a:b], vw[:, c:d], pw[:, c:d]], axis=1
            )

        rows = q1.shape[0]
        first, second = by_head(0), by_head(1)
        mine = core == 0
        wbuf[z, x, pl.ds(core * rows, rows), :] = jnp.where(mine, first, second)
        wsend[...] = jnp.where(mine, second, first)
        tokbuf[core, y] = tokens[...]
        qz[...] = jnp.zeros_like(qz)
        mbuf[...] = jnp.full(mbuf.shape, low_score, F32)
        lbuf[...] = jnp.zeros_like(lbuf)
        acc[...] = jnp.zeros_like(acc)

        barrier = pltpu.get_barrier_semaphore()
        neighbours = [at_z(1), at_z(-1), at_x(1), at_x(-1), at_y(1), at_y(-1), at_partner()]
        for device in neighbours:
            pl.semaphore_signal(barrier, inc=1, device_id=device, device_id_type=MESH)
        pl.semaphore_wait(barrier, len(neighbours))

        w_swap = post(
            remote(wsend, wbuf.at[z, x, pl.ds(core * rows, rows), :], at_partner())
        )
        half = tok // 2
        tok_ring = Ring(
            ys, y, at_y, lambda u, s: tokbuf.at[core, s, pl.ds(u * half, half), :], sems
        )
        tok_ring.begin()

        def share_tokens(s):
            return post(remote(tokbuf.at[core, s], tokbuf.at[core, s], at_partner()))

        shared = [share_tokens(y)]

        w_ring_x = Ring(
            xs, x, at_x, lambda u, s: wbuf.at[z, s, pl.ds(u * rows, rows), :], sems
        )
        w_ring_z = Ring(
            zs, z, at_z, lambda u, s: wbuf.at[s, pl.ds(u * (xs // 2), xs // 2)], sems
        )
        w_swap.wait_recv()
        w_ring_x.begin()

        eye = (
            lax.broadcasted_iota(jnp.int32, (rows, rows), 0)
            == lax.broadcasted_iota(jnp.int32, (rows, rows), 1)
        ).astype(BF16)
        oat = dot(eye, oa[...], ((1,), (1,))).astype(BF16)
        opt = dot(eye, op[...], ((1,), (1,))).astype(BF16)
        wt[z, x, core] = jnp.concatenate(
            [oat[:, :128], opt[:, :128], oat[:, 128:], opt[:, 128:]], axis=1
        )
        cb, sb = cos_far[pl.ds(place, 1), :], sin_far[pl.ds(place, 1), :]

        for h in range(1, xs // 2 + 1):
            w_ring_x.step(h)
        w_ring_z.begin()

        wt_half = rows // 2
        wt_ring_z = Ring(
            zs, z, at_z, lambda u, s: wt.at[s, x, core, pl.ds(u * wt_half, wt_half), :], sems
        )
        wt_ring_x = Ring(
            xs, x, at_x, lambda u, s: wt.at[pl.ds(u * (zs // 2), zs // 2), s, core], sems
        )

        for h in range(1, ys // 2 + 1):
            tok_ring.step(h)
            if h < ys // 2:
                shared.append(share_tokens(tok_ring.slot(0, h)))
                shared.append(share_tokens(tok_ring.slot(1, h)))
            else:
                shared.append(share_tokens(tok_ring.slot(0, h)))
        for copy in shared:
            copy.wait_recv()

        per_part = part // kb
        for owner in range(2):
            square = jnp.zeros((tok, 1), F32)
            for s in range(ys):
                block = tokbuf[owner, s].astype(F32)
                square = square + jnp.sum(block * block, axis=1, keepdims=True)
            scale = lax.rsqrt(square * (1.0 / wide) + norm_floor)
            for s in range(ys):
                block = tokbuf[owner, s].astype(F32) * scale * gain[:, s * part : (s + 1) * part]
                for j in range(per_part):
                    nrm[s * per_part + j, owner * tok : (owner + 1) * tok, :] = block[
                        :, j * kb : (j + 1) * kb
                    ].astype(BF16)

        def project(s, start):
            weight = wbuf[s].reshape(kz, 512)
            per_slot = kz // kb
            term = dot(nrm[s * per_slot], weight[0:kb])
            for j in range(1, per_slot):
                term = term + dot(nrm[s * per_slot + j], weight[j * kb : (j + 1) * kb])
            if start:
                proj[...] = term
            else:
                proj[...] += term

        project(z, True)
        for h in range(1, zs // 2 + 1):
            w_ring_z.step(h)
            project(w_ring_z.slot(0, h), False)
            if h < zs // 2:
                project(w_ring_z.slot(1, h), False)

        ca, sa = cos_near[...], sin_near[...]
        cosine = ca * cb - sa * sb
        sine = sa * cb + ca * sb
        low = lax.rem(lax.broadcasted_iota(jnp.int32, (chip, 128), 1), 64) < 32

        def turned(v):
            swapped = jnp.where(low, pltpu.roll(v, 96, 1), pltpu.roll(v, 32, 1))
            return v * cosine + swapped * sine

        kbuf[z] = turned(proj[:, 128:256]).astype(BF16)
        vbuf[z] = proj[:, 256:384].T.astype(BF16)
        kv_ring = Ring(
            zs, z, at_z, lambda u, s: (kbuf.at[s] if u == 0 else vbuf.at[s]), sems
        )
        kv_ring.begin()
        queries = (turned(proj[:, 0:128]) * (0.125 * math.log2(math.e))).T.astype(BF16)
        qz[x, 0:64, 0:chip] = queries[0:64]
        qz[x, 64:128, chip : 2 * chip] = queries[64:128]
        q_ring = Ring(
            xs, x, at_x,
            lambda u, s: qz.at[s, pl.ds(64 * u, 64), pl.ds(chip * u, chip)], sems,
        )
        q_ring.begin()

        pool = proj[:, 384:512].astype(BF16)
        pext[16 : 16 + chip, :] = pool.astype(F32)
        halo_x[0] = pool[chip - 16 :, :]
        to_x = post(remote(halo_x.at[0], halo_x.at[1], at_x(1)))
        wt_ring_z.begin()

        def tile(slot, ch, lt, masked):
            lanes = pl.ds(lt * LANE_TILE, LANE_TILE)
            s = dot(kbuf[slot], qz[ch, :, lanes])
            if masked:
                offset = (lt * LANE_TILE) % chip
                visible = lax.broadcasted_iota(jnp.int32, s.shape, 0) <= (
                    lax.broadcasted_iota(jnp.int32, s.shape, 1) + offset
                )
                s = jnp.where(visible, s, low_score)
            before = mbuf[ch, 0:1, lanes]
            now = jnp.maximum(before, jnp.max(s, axis=0, keepdims=True))
            p = jnp.exp2(s - now)
            factor = jnp.exp2(before - now)
            mbuf[ch, 0:1, lanes] = now
            lbuf[ch, 0:1, lanes] = lbuf[ch, 0:1, lanes] * factor + jnp.sum(
                p, axis=0, keepdims=True
            )
            acc[ch, :, lanes] = acc[ch, :, lanes] * factor + dot(vbuf[slot], p.astype(BF16))

        def attend(slot, start):
            def chunk(ch, carry):
                for lt in range(tiles):
                    tile(slot, ch, lt, False)
                return carry

            lax.fori_loop(start, xs, chunk, 0)

        for lt in range(tiles):
            tile(z, x, lt, True)

        to_x.wait_recv()
        to_z = post(remote(halo_x.at[1], halo_z, at_z(1)))
        for h in range(1, xs // 2 + 1):
            q_ring.step(h)
        to_z.wait_recv()
        from_x, from_z = halo_x[1].astype(F32), halo_z[...].astype(F32)
        prior = jnp.where(x == 0, from_z, from_x)
        pext[0:16, :] = jnp.where(place == 0, 0.0, prior)
        window = jnp.left_shift(2, lax.rem(head, 4))
        whole = pext[...]
        run = whole
        window_sum = jnp.zeros((chip, 128), F32)
        for k in range(4):
            lag = 1 << k
            run = run + jnp.concatenate(
                [jnp.zeros((lag, 128), F32), run[: 16 + chip - lag]], axis=0
            )
            window_sum = jnp.where(window == 2 * lag, run[16:], window_sum)
        position = place * chip + lax.broadcasted_iota(jnp.int32, (chip, 128), 0)
        count = jnp.minimum(position + 1, window).astype(F32)
        window_mean = (window_sum / count - whole[16:]).astype(BF16)
        pooled = (dot(window_mean, gw[head]) * pscale[pl.ds(head, 1), :]).astype(BF16)
        abuf[0, :, 128:256] = pooled[0:tok]
        abuf[1, :, 128:256] = pooled[tok:]
        attend(z, x + 1)

        for h in range(1, zs // 2 + 1):
            kv_ring.step(h)
            wt_ring_z.step(h)
            if h == zs // 2:
                wt_ring_x.begin()
            up, down = kv_ring.slot(0, h), kv_ring.slot(1, h)

            @pl.when(up < z)
            def _():
                attend(up, 0)

            if h < zs // 2:

                @pl.when(down < z)
                def _():
                    attend(down, 0)

        wt_shared = [
            post(remote(wt.at[:, x, core], wt.at[:, x, core], at_partner()))
        ]
        for h in range(1, xs // 2 + 1):
            wt_ring_x.step(h)
            for d in (0, 1):
                if h < xs // 2 or d == 0:
                    s = wt_ring_x.slot(d, h)
                    wt_shared.append(
                        post(remote(wt.at[:, s, core], wt.at[:, s, core], at_partner()))
                    )

        def share(ch, m):
            lanes = pl.ds(m * chip, chip)
            total = lbuf[ch, 0:1, lanes]
            some = total > 0.0
            safe = jnp.where(some, total, 1.0)
            weight = jnp.where(some, mbuf[ch, 0:1, lanes] + jnp.log2(safe), low_score)
            return acc[ch, :, lanes] * (1.0 / safe), weight

        def joined(*shares):
            top = shares[0][1]
            for _, weight in shares[1:]:
                top = jnp.maximum(top, weight)
            factors = [jnp.exp2(weight - top) for _, weight in shares]
            total = sum(factors)
            value = sum(o * f for (o, _), f in zip(shares, factors)) * (1.0 / total)
            return value, top + jnp.log2(total)

        def put(pair, o_ref, e_ref):
            o_ref[...] = pair[0].astype(BF16)
            e_ref[...] = jnp.broadcast_to(pair[1], e_ref.shape)

        def send_pair(o_src, e_src, o_dst, e_dst, device):
            return post(remote(o_src, o_dst, device)), post(remote(e_src, e_dst, device))

        def get(o_ref, e_ref):
            return o_ref[...].astype(F32), e_ref[0:1, :]

        ahead = lax.rem(x + 1, xs)
        behind = lax.rem(x + xs - 1, xs)
        across = lax.rem(x + 2, xs)
        sides = ((ahead, at_x(1)), (behind, at_x(-1)))
        first_hop = []
        for m in (0, 1):
            put(share(across, m), o1s.at[m], e1s.at[m])
            first_hop.append(
                send_pair(o1s.at[m], e1s.at[m], o1r.at[m], e1r.at[m], sides[m][1])
            )
        second_hop = []
        for m in (0, 1):
            chunk, device = sides[m]
            k = 1 - m
            put(share(chunk, k), o2s.at[m, k], e2s.at[m, k])
            second_hop.append(
                send_pair(o2s.at[m, k], e2s.at[m, k], o2r.at[m, k], e2r.at[m, k], device)
            )
        for m in (0, 1):
            for copy in first_hop[m]:
                copy.wait_recv()
            chunk, device = sides[m]
            put(joined(share(chunk, m), get(o1r.at[m], e1r.at[m])), o2s.at[m, m], e2s.at[m, m])
            second_hop.append(
                send_pair(o2s.at[m, m], e2s.at[m, m], o2r.at[m, m], e2r.at[m, m], device)
            )
        for pair in second_hop:
            for copy in pair:
                copy.wait_recv()
        means = [
            joined(
                share(x, m),
                get(o2r.at[0, m], e2r.at[0, m]),
                get(o2r.at[1, m], e2r.at[1, m]),
            )[0]
            for m in (0, 1)
        ]
        difference = means[0] - lam[head] * means[1]
        norm = lax.rsqrt(jnp.mean(difference * difference, axis=0, keepdims=True) + head_floor)
        attn = ((difference * norm).T * hgain[...] * head_scale).astype(BF16)

        abuf[0, :, 0:128] = attn[0:tok]
        abuf[1, :, 0:128] = attn[tok:]
        swap = post(remote(abuf.at[other], abuf.at[2], at_partner()))
        swap.wait_recv()
        for copy in wt_shared:
            copy.wait_recv()

        own_rows = abuf[core]
        their_rows = abuf[2]
        rows_0 = jnp.where(core == 0, own_rows, their_rows)
        rows_1 = jnp.where(core == 0, their_rows, own_rows)
        per_z = wide // zs
        for s in range(zs):
            weight = wt[s].reshape(per_z, 512)
            ysum[:, s * per_z : (s + 1) * per_z] = (
                dot(rows_0, weight[:, 0:256], ((1,), (1,)))
                + dot(rows_1, weight[:, 256:512], ((1,), (1,)))
            ).astype(BF16)

        y_half = quarter // 2
        y_across = lax.rem(y + 2, ys)
        y_sides = (
            (lax.rem(y + 1, ys), at_y(1)),
            (lax.rem(y + ys - 1, ys), at_y(-1)),
        )

        def rows_of(target, m):
            return pl.ds(target * quarter + m * y_half, y_half)

        y_first, y_second = [], []
        for m in (0, 1):
            y_first.append(
                post(remote(ysum.at[rows_of(y_across, m), :], y1r.at[m], y_sides[m][1]))
            )
        for m in (0, 1):
            target, device = y_sides[m]
            y_second.append(
                post(remote(ysum.at[rows_of(target, 1 - m), :], y2r.at[m, 1 - m], device))
            )
        for m in (0, 1):
            target, device = y_sides[m]
            y_first[m].wait_recv()
            y2s[m] = (
                ysum[rows_of(target, m), :].astype(F32) + y1r[m].astype(F32)
            ).astype(BF16)
            y_second.append(post(remote(y2s.at[m], y2r.at[m, m], device)))
        for copy in y_second:
            copy.wait_recv()
        for m in (0, 1):
            out[m * y_half : (m + 1) * y_half, :] = (
                ysum[rows_of(y, m), :].astype(F32)
                + y2r[0, m].astype(F32)
                + y2r[1, m].astype(F32)
            ).astype(BF16)

        for copy in sent:
            copy.wait_send()
        for ring in (tok_ring, w_ring_x, w_ring_z, wt_ring_x, wt_ring_z, kv_ring, q_ring):
            ring.finish()

    return kernel


def solution(mesh):
    sp_size, ys = mesh.shape["sp"], mesh.shape["tp"]
    zs, xs = Z_SIZE, X_SIZE
    assert zs * xs * 2 == sp_size

    def body(
        tokens, norm_gain, query_one, key_one, query_two, key_two, value_weight, pool_weight,
        lambda_head, head_gain, group_weight, pool_scale, out_attn, out_pool,
    ):
        tok, part = tokens.shape
        wide = part * ys
        chip = 2 * tok
        rows = query_one.shape[0]
        quarter = tok // ys
        tables = rope_tables(chip, zs * xs)
        vmem = pl.BlockSpec(memory_space=pltpu.VMEM)
        smem = pl.BlockSpec(memory_space=pltpu.SMEM)
        args = (
            tokens, norm_gain.reshape(1, wide), query_one, key_one, query_two, key_two,
            value_weight, pool_weight, lambda_head, head_gain.reshape(1, 128), group_weight,
            pool_scale.reshape(-1, 128), out_attn, out_pool, *tables,
        )
        specs = [vmem] * len(args)
        specs[8] = smem
        semaphores = 128
        return pl.pallas_call(
            make_kernel(zs, xs, ys, tok, wide),
            out_shape=jax.ShapeDtypeStruct((quarter, wide), BF16),
            in_specs=specs,
            out_specs=vmem,
            scratch_shapes=[
                pltpu.VMEM((rows, 512), BF16),
                pltpu.VMEM((zs, xs, 2 * rows, 512), BF16),
                pltpu.VMEM((zs, xs, 2, rows, 512), BF16),
                pltpu.VMEM((2, ys, tok, part), BF16),
                pltpu.VMEM((max(zs, ys), chip, wide // max(zs, ys)), BF16),
                pltpu.VMEM((chip, 512), F32),
                pltpu.VMEM((zs, chip, 128), BF16),
                pltpu.VMEM((zs, 128, chip), BF16),
                pltpu.VMEM((xs, 128, 2 * chip), BF16),
                pltpu.VMEM((xs, 128, 2 * chip), F32),
                pltpu.VMEM((xs, 8, 2 * chip), F32),
                pltpu.VMEM((xs, 8, 2 * chip), F32),
                pltpu.VMEM((16 + chip, 128), F32),
                pltpu.VMEM((2, 16, 128), BF16),
                pltpu.VMEM((16, 128), BF16),
                pltpu.VMEM((2, 128, chip), BF16),
                pltpu.VMEM((2, 8, chip), F32),
                pltpu.VMEM((2, 128, chip), BF16),
                pltpu.VMEM((2, 8, chip), F32),
                pltpu.VMEM((2, 2, 128, chip), BF16),
                pltpu.VMEM((2, 2, 8, chip), F32),
                pltpu.VMEM((2, 2, 128, chip), BF16),
                pltpu.VMEM((2, 2, 8, chip), F32),
                pltpu.VMEM((3, tok, 256), BF16),
                pltpu.VMEM((tok, wide), BF16),
                pltpu.VMEM((2, quarter // 2, wide), BF16),
                pltpu.VMEM((2, quarter // 2, wide), BF16),
                pltpu.VMEM((2, 2, quarter // 2, wide), BF16),
                pltpu.SemaphoreType.DMA((semaphores,)),
                pltpu.SemaphoreType.DMA((semaphores,)),
            ],
            compiler_params=pltpu.CompilerParams(
                collective_id=0, has_side_effects=True, vmem_limit_bytes=60 * 1024 * 1024
            ),
            name="mixer",
        )(*args)

    in_specs = (
        P("sp", "tp"),
        P(),
        P("sp", "tp"),
        P("sp", "tp"),
        P("sp", "tp"),
        P("sp", "tp"),
        P("sp", "tp"),
        P("sp", "tp"),
        P(),
        P(),
        P(),
        P(),
        P("tp", "sp"),
        P("tp", "sp"),
    )
    out_specs = P(("sp", "tp"), None)
    return jax.shard_map(body, mesh=mesh, in_specs=in_specs, out_specs=out_specs, check_vma=False)
```

```python
import math

import jax
import jax.numpy as jnp
import numpy as np
from jax import lax
from jax.experimental import pallas as pl
from jax.experimental.pallas import tpu as pltpu
from jax.sharding import PartitionSpec as P

MESH = pl.DeviceIdType.MESH
F32 = jnp.float32
BF16 = jnp.bfloat16
Z_SIZE = 8
X_SIZE = 4
LANE_TILE = 256

rope_base = 500000.0
head_scale = 0.8
norm_floor = 1e-06
head_floor = 0.001
low_score = -1e30


def rope_tables(chip_tokens, chips):
    lane = np.arange(128)
    inverse = rope_base ** (-((lane % 32) * 2.0 / 64.0))
    sign = np.where(lane % 64 < 32, -1.0, 1.0)
    near = np.arange(chip_tokens)[:, None] * inverse[None, :]
    far = (np.arange(chips) * chip_tokens)[:, None] * inverse[None, :]
    return (
        np.cos(near).astype(np.float32),
        (np.sin(near) * sign).astype(np.float32),
        np.cos(far).astype(np.float32),
        (np.sin(far) * sign).astype(np.float32),
    )


class Ring:
    def __init__(self, n, me, device, unit, sems):
        self.n, self.me, self.device, self.unit = n, me, device, unit
        self.sems = {}
        for h in range(1, n // 2 + 1):
            for d in (0, 1):
                for u in (0, 1):
                    if self.has(d, h, u):
                        self.sems[d, h, u] = sems()

    def has(self, d, h, u):
        return h < self.n // 2 or (h == self.n // 2 and d == u)

    def slot(self, d, h):
        sign = 1 if d == 0 else -1
        return lax.rem(self.me - sign * h + self.n, self.n)

    def copy(self, d, h, u, slot):
        ref = self.unit(u, slot)
        send_sem, recv_sem = self.sems[d, h, u]
        return pltpu.make_async_remote_copy(
            src_ref=ref,
            dst_ref=ref,
            send_sem=send_sem,
            recv_sem=recv_sem,
            device_id=self.device(1 if d == 0 else -1),
            device_id_type=MESH,
        )

    def send(self, d, h, u):
        self.copy(d, h, u, self.slot(d, h - 1)).start()

    def begin(self, units=(0, 1)):
        for u in units:
            for d in (0, 1):
                if self.has(d, 1, u):
                    self.send(d, 1, u)

    def step(self, h):
        for u in (0, 1):
            for d in (0, 1):
                if self.has(d, h, u):
                    self.copy(d, h, u, self.slot(d, h)).wait_recv()
                    if (d, h + 1, u) in self.sems:
                        self.send(d, h + 1, u)

    def finish(self):
        for d, h, u in self.sems:
            self.copy(d, h, u, self.slot(d, h - 1)).wait_send()


def dot(a, b, dims=((1,), (0,))):
    return lax.dot_general(a, b, (dims, ((), ())), preferred_element_type=F32)


def make_kernel(zs, xs, ys, tok, wide):
    chip = 2 * tok
    part = wide // ys
    quarter = tok // ys
    tiles = 2 * chip // LANE_TILE

    def kernel(
        tokens, gain, q1, k1, q2, k2, vw, pw, lam, hgain, gw, pscale, oa, op,
        cos_near, sin_near, cos_far, sin_far,
        out,
        wsend, wbuf, wt, tokbuf, nrm, proj, kbuf, vbuf, qz, acc, mbuf, lbuf,
        pext, halo, o1s, e1s, o1r, e1r, o2s, e2s, o2r, e2r, abuf,
        ysum, y1r, y2s, y2r, send_sems, recv_sems,
    ):
        sp = lax.axis_index("sp")
        y = lax.axis_index("tp")
        core = lax.rem(sp, 2)
        place = sp // 2
        x = lax.rem(place, xs)
        z = place // xs
        other = 1 - core
        head = 2 * y + core

        def at_z(step):
            return {"sp": (lax.rem(z + step + zs, zs) * xs + x) * 2 + core, "tp": y}

        def at_x(step):
            return {"sp": (z * xs + lax.rem(x + step + xs, xs)) * 2 + core, "tp": y}

        def at_y(step):
            return {"sp": sp, "tp": lax.rem(y + step + ys, ys)}

        def at_chip(step):
            chips = zs * xs
            return {"sp": lax.rem(place + step + chips, chips) * 2 + core, "tp": y}

        def at_partner():
            return {"sp": place * 2 + other, "tp": y}

        used = [0]

        def sems():
            k = used[0]
            used[0] += 1
            return send_sems.at[k], recv_sems.at[k]

        def remote(src, dst, device):
            send_sem, recv_sem = sems()
            return pltpu.make_async_remote_copy(
                src_ref=src, dst_ref=dst, send_sem=send_sem, recv_sem=recv_sem,
                device_id=device, device_id_type=MESH,
            )

        sent = []

        def post(copy):
            copy.start()
            sent.append(copy)
            return copy

        def by_head(h):
            a, b = h * 64, h * 64 + 64
            c, d = h * 128, h * 128 + 128
            return jnp.concatenate(
                [q1[:, a:b], q2[:, a:b], k1[:, a:b], k2[:, a:b], vw[:, c:d], pw[:, c:d]], axis=1
            )

        rows = q1.shape[0]
        first, second = by_head(0), by_head(1)
        mine = core == 0
        own_rows = pl.ds(core * rows, rows)
        their_rows = pl.ds(other * rows, rows)
        wbuf[z, x, own_rows, :] = jnp.where(mine, first, second)
        wsend[...] = jnp.where(mine, second, first)
        tokbuf[core, y] = tokens[...]
        wt[z, x, core] = jnp.concatenate(
            [oa[:, :128], op[:, :128], oa[:, 128:], op[:, 128:]], axis=1
        )
        qz[...] = jnp.zeros_like(qz)
        mbuf[...] = jnp.full(mbuf.shape, low_score, F32)
        lbuf[...] = jnp.zeros_like(lbuf)
        acc[...] = jnp.zeros_like(acc)

        barrier = pltpu.get_barrier_semaphore()
        neighbours = [
            at_z(1), at_z(-1), at_x(1), at_x(-1), at_y(1), at_y(-1), at_partner(), at_chip(1), at_chip(-1),
        ]
        for device in neighbours:
            pl.semaphore_signal(barrier, inc=1, device_id=device, device_id_type=MESH)
        pl.semaphore_wait(barrier, len(neighbours))

        w_swap = post(remote(wsend, wbuf.at[z, x, own_rows, :], at_partner()))
        half = tok // 2
        strip = rows // 2
        tok_ring = Ring(
            ys, y, at_y, lambda u, s: tokbuf.at[core, s, pl.ds(u * half, half), :], sems
        )
        own_x = Ring(
            xs, x, at_x,
            lambda u, s: wbuf.at[z, s, pl.ds(core * rows + u * strip, strip), :], sems,
        )
        own_z = Ring(
            zs, z, at_z,
            lambda u, s: wbuf.at[s, pl.ds(u * (xs // 2), xs // 2), own_rows, :], sems,
        )
        their_z = Ring(
            zs, z, at_z,
            lambda u, s: wbuf.at[s, x, pl.ds(other * rows + u * strip, strip), :], sems,
        )
        wt_ring_z = Ring(
            zs, z, at_z, lambda u, s: wt.at[s, x, core, pl.ds(u * strip, strip), :], sems
        )
        wt_ring_x = Ring(
            xs, x, at_x, lambda u, s: wt.at[pl.ds(u * (zs // 2), zs // 2), s, core], sems
        )

        def their_x_ring(slot):
            ring = Ring(
                xs, x, at_x,
                lambda u, s: wbuf.at[slot, s, pl.ds(other * rows + u * strip, strip), :], sems,
            )
            ring.begin()
            return ring

        own_x.begin()
        tok_ring.begin()

        def share_tokens(s):
            return post(remote(tokbuf.at[core, s], tokbuf.at[core, s], at_partner()))

        shared = [share_tokens(y)]
        cb, sb = cos_far[pl.ds(place, 1), :], sin_far[pl.ds(place, 1), :]
        w_swap.wait_recv()
        their_z.begin()
        their_x = [their_x_ring(z)]

        def their_step(h):
            their_z.step(h)
            their_x.append(their_x_ring(their_z.slot(0, h)))
            if h < zs // 2:
                their_x.append(their_x_ring(their_z.slot(1, h)))

        def tok_step(h):
            tok_ring.step(h)
            shared.append(share_tokens(tok_ring.slot(0, h)))
            if h < ys // 2:
                shared.append(share_tokens(tok_ring.slot(1, h)))

        own_x.step(1)
        their_step(1)
        own_x.step(2)
        own_z.begin()
        if zs > 2:
            their_step(2)
            their_step(3)
        tok_step(1)
        for ring in their_x[:3]:
            ring.step(1)
        if zs > 2:
            their_step(4)
        own_z.step(1)
        wt_ring_z.begin()
        for ring in their_x[:3]:
            ring.step(2)
        tok_step(2)
        for copy in shared:
            copy.wait_recv()

        for owner in range(2):
            square = jnp.zeros((tok, 1), F32)
            for s in range(ys):
                block = tokbuf[owner, s].astype(F32)
                square = square + jnp.sum(block * block, axis=1, keepdims=True)
            scale = lax.rsqrt(square * (1.0 / wide) + norm_floor)
            for s in range(ys):
                block = tokbuf[owner, s].astype(F32) * scale * gain[:, s * part : (s + 1) * part]
                nrm[owner * tok : (owner + 1) * tok, s * part : (s + 1) * part] = block.astype(BF16)

        wt_hops = list(range(1, zs // 2 + 1))

        def wt_next():
            if wt_hops:
                wt_ring_z.step(wt_hops.pop(0))

        if zs > 2:
            own_z.step(2)
            for ring in their_x[3:]:
                ring.step(1)
            wt_next()
            own_z.step(3)
            for ring in their_x[3:]:
                ring.step(2)
            wt_next()
            own_z.step(4)
        weight = wbuf[...].reshape(wide, 512)
        for cut in range(0, 512, 256):
            proj[:, cut : cut + 256] = dot(nrm[...], weight[:, cut : cut + 256])
        ca, sa = cos_near[...], sin_near[...]
        cosine = ca * cb - sa * sb
        sine = sa * cb + ca * sb
        low = lax.rem(lax.broadcasted_iota(jnp.int32, (chip, 128), 1), 64) < 32

        def turned(v):
            swapped = jnp.where(low, pltpu.roll(v, 96, 1), pltpu.roll(v, 32, 1))
            return v * cosine + swapped * sine

        pool = proj[:, 384:512].astype(BF16)
        pext[16 : 16 + chip, :] = pool.astype(F32)
        halo[0] = pool[chip - 16 :, :]
        to_next = post(remote(halo.at[0], halo.at[1], at_chip(1)))
        kbuf[z] = turned(proj[:, 128:256]).astype(BF16)
        vbuf[z] = proj[:, 256:384].T.astype(BF16)

        def kv_copy(d, h, u, slot):
            ref = kbuf.at[slot] if u == 0 else vbuf.at[slot]
            k = kv_first + (h - 1) * 4 + d * 2 + u
            return pltpu.make_async_remote_copy(
                src_ref=ref, dst_ref=ref, send_sem=send_sems.at[k], recv_sem=recv_sems.at[k],
                device_id=at_z(1 if d == 0 else -1), device_id_type=MESH,
            )

        kv_first = used[0]
        used[0] += 2 * zs
        last = zs // 2

        def kv_slot(d, h):
            return lax.rem(z + (h if d else -h) + zs, zs)

        def kv_step(h):
            for u in (0, 1):
                for d in (0, 1):

                    @pl.when((h < last) | (d == u))
                    def _():
                        kv_copy(d, h, u, kv_slot(d, h)).wait_recv()

                        @pl.when((h + 1 < last) | ((h + 1 == last) & (d == u)))
                        def _():
                            kv_copy(d, h + 1, u, kv_slot(d, h)).start()

        for u in (0, 1):
            for d in (0, 1):
                if last > 1 or d == u:
                    kv_copy(d, 1, u, z).start()
        queries = (turned(proj[:, 0:128]) * (0.125 * math.log2(math.e))).T.astype(BF16)
        qz[x, 0:64, 0:chip] = queries[0:64]
        qz[x, 64:128, chip : 2 * chip] = queries[64:128]
        q_ring = Ring(
            xs, x, at_x,
            lambda u, s: qz.at[s, pl.ds(64 * u, 64), pl.ds(chip * u, chip)], sems,
        )
        q_ring.begin()

        def attend(slot, chunks, masked=False):
            todo = [(ch, lt) for ch in chunks for lt in range(tiles)]

            def lanes_of(lt):
                return pl.ds(lt * LANE_TILE, LANE_TILE)

            def scores(ch, lt):
                return dot(kbuf[slot], qz[ch, :, lanes_of(lt)])

            def add_values(ch, lt, factor, p):
                lanes = lanes_of(lt)
                acc[ch, :, lanes] = acc[ch, :, lanes] * factor + dot(vbuf[slot], p)

            ready = [scores(*item) for item in todo[:2]]
            pending = None
            for k, (ch, lt) in enumerate(todo):
                if k + 2 < len(todo):
                    ready.append(scores(*todo[k + 2]))
                s = ready.pop(0)
                lanes = lanes_of(lt)
                if masked:
                    offset = (lt * LANE_TILE) % chip
                    visible = lax.broadcasted_iota(jnp.int32, s.shape, 0) <= (
                        lax.broadcasted_iota(jnp.int32, s.shape, 1) + offset
                    )
                    s = jnp.where(visible, s, low_score)
                before = mbuf[ch, 0:1, lanes]
                now = jnp.maximum(before, jnp.max(s, axis=0, keepdims=True))
                p = jnp.exp2(s - now)
                factor = jnp.exp2(before - now)
                mbuf[ch, 0:1, lanes] = now
                lbuf[ch, 0:1, lanes] = lbuf[ch, 0:1, lanes] * factor + jnp.sum(
                    p, axis=0, keepdims=True
                )
                if pending is not None:
                    add_values(*pending)
                pending = (ch, lt, factor, p.astype(BF16))
            add_values(*pending)

        attend(z, [x], True)
        q_ring.step(1)
        wt_next()
        q_ring.step(2)
        lax.fori_loop(x + 1, xs, lambda ch, carry: (attend(z, [ch]), carry)[1], 0)
        wt_next()
        wt_ring_x.begin()
        to_next.wait_recv()
        prior = halo[1].astype(F32)
        pext[0:16, :] = jnp.where(place == 0, 0.0, prior)
        window = jnp.left_shift(2, lax.rem(head, 4))
        whole = pext[...]
        run = whole
        window_sum = jnp.zeros((chip, 128), F32)
        for k in range(4):
            lag = 1 << k
            run = run + jnp.concatenate(
                [jnp.zeros((lag, 128), F32), run[: 16 + chip - lag]], axis=0
            )
            window_sum = jnp.where(window == 2 * lag, run[16:], window_sum)
        position = place * chip + lax.broadcasted_iota(jnp.int32, (chip, 128), 0)
        count = jnp.minimum(position + 1, window).astype(F32)
        window_mean = (window_sum / count - whole[16:]).astype(BF16)
        pooled = (dot(window_mean, gw[head]) * pscale[pl.ds(head, 1), :]).astype(BF16)
        abuf[0, :, 128:256] = pooled[0:tok]
        abuf[1, :, 128:256] = pooled[tok:]
        wt_slots = [x, *(wt_ring_x.slot(d, h) for h in range(1, xs // 2) for d in (0, 1))]
        wt_slots.append(wt_ring_x.slot(0, xs // 2))
        wt_shared = [
            remote(wt.at[:, s, core], wt.at[:, s, core], at_partner()) for s in wt_slots
        ]
        sent.extend(wt_shared)
        wt_shared[0].start()

        def wt_step(h):
            wt_ring_x.step(h)
            for copy in wt_shared[1:3] if h == 1 else wt_shared[3:]:
                copy.start()

        def arrival(k, carry):
            h, d = k // 2 + 1, lax.rem(k, 2)

            @pl.when(d == 0)
            def _():
                kv_step(h)

            if zs > 2:
                for hop in range(1, xs // 2 + 1):

                    @pl.when(k == 2 * hop)
                    def _():
                        wt_step(hop)

            slot = lax.rem(z + jnp.where(d == 0, -h, h) + zs, zs)

            @pl.when(slot < z)
            def _():
                attend(slot, range(xs))

            return carry

        lax.fori_loop(0, zs - 1, arrival, 0)
        if zs == 2:
            wt_step(1)
            wt_step(2)

        def share(ch, m):
            lanes = pl.ds(m * chip, chip)
            total = lbuf[ch, 0:1, lanes]
            some = total > 0.0
            safe = jnp.where(some, total, 1.0)
            weight = jnp.where(some, mbuf[ch, 0:1, lanes] + jnp.log2(safe), low_score)
            return acc[ch, :, lanes] * (1.0 / safe), weight

        def joined(*shares):
            top = shares[0][1]
            for _, weight in shares[1:]:
                top = jnp.maximum(top, weight)
            factors = [jnp.exp2(weight - top) for _, weight in shares]
            total = sum(factors)
            value = sum(o * f for (o, _), f in zip(shares, factors)) * (1.0 / total)
            return value, top + jnp.log2(total)

        def put(pair, o_ref, e_ref):
            o_ref[...] = pair[0].astype(BF16)
            e_ref[...] = jnp.broadcast_to(pair[1], e_ref.shape)

        def send_pair(o_src, e_src, o_dst, e_dst, device):
            return post(remote(o_src, o_dst, device)), post(remote(e_src, e_dst, device))

        def get(o_ref, e_ref):
            return o_ref[...].astype(F32), e_ref[0:1, :]

        ahead = lax.rem(x + 1, xs)
        behind = lax.rem(x + xs - 1, xs)
        across = lax.rem(x + 2, xs)
        sides = ((ahead, at_x(1)), (behind, at_x(-1)))
        first_hop = []
        for m in (0, 1):
            put(share(across, m), o1s.at[m], e1s.at[m])
            first_hop.append(
                send_pair(o1s.at[m], e1s.at[m], o1r.at[m], e1r.at[m], sides[m][1])
            )
        second_hop = []
        for m in (0, 1):
            chunk, device = sides[m]
            k = 1 - m
            put(share(chunk, k), o2s.at[m, k], e2s.at[m, k])
            second_hop.append(
                send_pair(o2s.at[m, k], e2s.at[m, k], o2r.at[m, k], e2r.at[m, k], device)
            )
        for m in (0, 1):
            for copy in first_hop[m]:
                copy.wait_recv()
            chunk, device = sides[m]
            put(joined(share(chunk, m), get(o1r.at[m], e1r.at[m])), o2s.at[m, m], e2s.at[m, m])
            second_hop.append(
                send_pair(o2s.at[m, m], e2s.at[m, m], o2r.at[m, m], e2r.at[m, m], device)
            )
        for pair in second_hop:
            for copy in pair:
                copy.wait_recv()
        means = [
            joined(
                share(x, m),
                get(o2r.at[0, m], e2r.at[0, m]),
                get(o2r.at[1, m], e2r.at[1, m]),
            )[0]
            for m in (0, 1)
        ]
        difference = means[0] - lam[head] * means[1]
        norm = lax.rsqrt(jnp.mean(difference * difference, axis=0, keepdims=True) + head_floor)
        attn = ((difference * norm).T * hgain[...] * head_scale).astype(BF16)

        abuf[0, :, 0:128] = attn[0:tok]
        abuf[1, :, 0:128] = attn[tok:]
        swap = post(remote(abuf.at[other], abuf.at[2], at_partner()))
        swap.wait_recv()
        for copy in wt_shared:
            copy.wait_recv()

        rows_0 = jnp.where(core == 0, abuf[core], abuf[2])
        rows_1 = jnp.where(core == 0, abuf[2], abuf[core])
        per_z = wide // zs
        for s in range(zs):
            weight = wt[s].reshape(per_z, 512)
            ysum[:, s * per_z : (s + 1) * per_z] = (
                dot(rows_0, weight[:, 0:256], ((1,), (1,)))
                + dot(rows_1, weight[:, 256:512], ((1,), (1,)))
            ).astype(BF16)

        y_half = quarter // 2
        y_across = lax.rem(y + 2, ys)
        y_sides = (
            (lax.rem(y + 1, ys), at_y(1)),
            (lax.rem(y + ys - 1, ys), at_y(-1)),
        )

        def rows_of(target, m):
            return pl.ds(target * quarter + m * y_half, y_half)

        y_first, y_second = [], []
        for m in (0, 1):
            y_first.append(
                post(remote(ysum.at[rows_of(y_across, m), :], y1r.at[m], y_sides[m][1]))
            )
        for m in (0, 1):
            target, device = y_sides[m]
            y_second.append(
                post(remote(ysum.at[rows_of(target, 1 - m), :], y2r.at[m, 1 - m], device))
            )
        for m in (0, 1):
            target, device = y_sides[m]
            y_first[m].wait_recv()
            y2s[m] = (
                ysum[rows_of(target, m), :].astype(F32) + y1r[m].astype(F32)
            ).astype(BF16)
            y_second.append(post(remote(y2s.at[m], y2r.at[m, m], device)))
        for copy in y_second:
            copy.wait_recv()
        for m in (0, 1):
            out[m * y_half : (m + 1) * y_half, :] = (
                ysum[rows_of(y, m), :].astype(F32)
                + y2r[0, m].astype(F32)
                + y2r[1, m].astype(F32)
            ).astype(BF16)

        for copy in sent:
            copy.wait_send()
        for ring in (tok_ring, own_x, own_z, their_z, *their_x, wt_ring_x, wt_ring_z, q_ring):
            ring.finish()
        for h in range(1, last + 1):
            for d in (0, 1):
                for u in (0, 1):
                    if h < last or d == u:
                        kv_copy(d, h, u, kv_slot(d, h - 1)).wait_send()

    return kernel


def solution(mesh):
    sp_size, ys = mesh.shape["sp"], mesh.shape["tp"]
    zs, xs = Z_SIZE, X_SIZE
    assert zs * xs * 2 == sp_size

    def body(
        tokens, norm_gain, query_one, key_one, query_two, key_two, value_weight, pool_weight,
        lambda_head, head_gain, group_weight, pool_scale, out_attn, out_pool,
    ):
        tok, part = tokens.shape
        wide = part * ys
        chip = 2 * tok
        rows = query_one.shape[0]
        quarter = tok // ys
        tables = rope_tables(chip, zs * xs)
        vmem = pl.BlockSpec(memory_space=pltpu.VMEM)
        smem = pl.BlockSpec(memory_space=pltpu.SMEM)
        args = (
            tokens, norm_gain.reshape(1, wide), query_one, key_one, query_two, key_two,
            value_weight, pool_weight, lambda_head, head_gain.reshape(1, 128), group_weight,
            pool_scale.reshape(-1, 128), out_attn.T, out_pool.T, *tables,
        )
        specs = [vmem] * len(args)
        specs[8] = smem
        semaphores = 192
        return pl.pallas_call(
            make_kernel(zs, xs, ys, tok, wide),
            out_shape=jax.ShapeDtypeStruct((quarter, wide), BF16),
            in_specs=specs,
            out_specs=vmem,
            scratch_shapes=[
                pltpu.VMEM((rows, 512), BF16),
                pltpu.VMEM((zs, xs, 2 * rows, 512), BF16),
                pltpu.VMEM((zs, xs, 2, rows, 512), BF16),
                pltpu.VMEM((2, ys, tok, part), BF16),
                pltpu.VMEM((chip, wide), BF16),
                pltpu.VMEM((chip, 512), F32),
                pltpu.VMEM((zs, chip, 128), BF16),
                pltpu.VMEM((zs, 128, chip), BF16),
                pltpu.VMEM((xs, 128, 2 * chip), BF16),
                pltpu.VMEM((xs, 128, 2 * chip), F32),
                pltpu.VMEM((xs, 8, 2 * chip), F32),
                pltpu.VMEM((xs, 8, 2 * chip), F32),
                pltpu.VMEM((16 + chip, 128), F32),
                pltpu.VMEM((2, 16, 128), BF16),
                pltpu.VMEM((2, 128, chip), BF16),
                pltpu.VMEM((2, 8, chip), F32),
                pltpu.VMEM((2, 128, chip), BF16),
                pltpu.VMEM((2, 8, chip), F32),
                pltpu.VMEM((2, 2, 128, chip), BF16),
                pltpu.VMEM((2, 2, 8, chip), F32),
                pltpu.VMEM((2, 2, 128, chip), BF16),
                pltpu.VMEM((2, 2, 8, chip), F32),
                pltpu.VMEM((3, tok, 256), BF16),
                pltpu.VMEM((tok, wide), BF16),
                pltpu.VMEM((2, quarter // 2, wide), BF16),
                pltpu.VMEM((2, quarter // 2, wide), BF16),
                pltpu.VMEM((2, 2, quarter // 2, wide), BF16),
                pltpu.SemaphoreType.DMA((semaphores,)),
                pltpu.SemaphoreType.DMA((semaphores,)),
            ],
            compiler_params=pltpu.CompilerParams(
                collective_id=0, has_side_effects=True, vmem_limit_bytes=60 * 1024 * 1024
            ),
            name="mixer",
        )(*args)

    in_specs = (
        P("sp", "tp"),
        P(),
        P("sp", "tp"),
        P("sp", "tp"),
        P("sp", "tp"),
        P("sp", "tp"),
        P("sp", "tp"),
        P("sp", "tp"),
        P(),
        P(),
        P(),
        P(),
        P("tp", "sp"),
        P("tp", "sp"),
    )
    out_specs = P(("sp", "tp"), None)
    return jax.shard_map(body, mesh=mesh, in_specs=in_specs, out_specs=out_specs, check_vma=False)
```

```python
import math

import jax
import jax.numpy as jnp
import numpy as np
from jax import lax
from jax.experimental import pallas as pl
from jax.experimental.pallas import tpu as pltpu
from jax.sharding import PartitionSpec as P

MESH = pl.DeviceIdType.MESH
F32 = jnp.float32
BF16 = jnp.bfloat16
Z_SIZE = 8
X_SIZE = 4
LANE_TILE = 256
SEND_SEMAPHORES = 32
RECV_SEMAPHORES = 128

rope_base = 500000.0
head_scale = 0.8
norm_floor = 1e-06
head_floor = 0.001
low_score = -1e30


def rope_tables(chip_tokens, chips):
    lane = np.arange(128)
    inverse = rope_base ** (-((lane % 32) * 2.0 / 64.0))
    sign = np.where(lane % 64 < 32, -1.0, 1.0)
    near = np.arange(chip_tokens)[:, None] * inverse[None, :]
    far = (np.arange(chips) * chip_tokens)[:, None] * inverse[None, :]
    return (
        np.cos(near).astype(np.float32),
        (np.sin(near) * sign).astype(np.float32),
        np.cos(far).astype(np.float32),
        (np.sin(far) * sign).astype(np.float32),
    )


class Ring:
    def __init__(self, n, me, device, unit, send_sem, recv_sem, whole=False):
        self.n, self.me, self.device, self.unit, self.whole = n, me, device, unit, whole
        self.send_sem = send_sem
        self.recv = {(d, h, p): recv_sem() for h in range(1, n // 2 + 1) for d in (0, 1) for p in self.parts(d, h)}

    def parts(self, d, h):
        if h == self.n // 2:
            return (d,)
        return (None,) if self.whole else (0, 1)

    def slot(self, d, h):
        return lax.rem(self.me + (h if d else -h) + self.n, self.n)

    def copy(self, d, h, p, slot):
        ref = self.unit(p, slot)
        return pltpu.make_async_remote_copy(
            src_ref=ref,
            dst_ref=ref,
            send_sem=self.send_sem,
            recv_sem=self.recv[d, h, p],
            device_id=self.device(-1 if d else 1),
            device_id_type=MESH,
        )

    def send(self, d, h, p):
        self.copy(d, h, p, self.slot(d, h - 1)).start()

    def begin(self):
        for d in (0, 1):
            for p in self.parts(d, 1):
                self.send(d, 1, p)

    def step(self, h):
        units = (None,) if self.whole else (0, 1)
        for p in units if h < self.n // 2 else (0, 1):
            for d in (0, 1):
                if p in self.parts(d, h):
                    self.copy(d, h, p, self.slot(d, h)).wait_recv()
                    if h + 1 < self.n // 2:
                        self.send(d, h + 1, p)
                    elif h + 1 == self.n // 2 and p in (None, d):
                        self.send(d, h + 1, d)

    def sent_bytes(self, slot_bytes):
        return sum(slot_bytes if p is None else slot_bytes // 2 for _, _, p in self.recv)


def dot(a, b, dims=((1,), (0,))):
    return lax.dot_general(a, b, (dims, ((), ())), preferred_element_type=F32)


def make_kernel(zs, xs, ys, tok, wide):
    chip = 2 * tok
    part = wide // ys
    quarter = tok // ys
    tiles = 2 * chip // LANE_TILE

    def kernel(
        tokens, gain, q1, k1, q2, k2, vw, pw, lam, hgain, gw, pscale, oa, op,
        cos_near, sin_near, cos_far, sin_far,
        out,
        wsend, wbuf, wt, tokbuf, nrm, proj, kbuf, vbuf, qz, acc, mbuf, lbuf,
        pext, halo, o1s, e1s, o1r, e1r, o2s, e2s, o2r, e2r, abuf,
        ysum, y1r, y2s, y2r, send_sems, recv_sems,
    ):
        sp = lax.axis_index("sp")
        y = lax.axis_index("tp")
        core = lax.rem(sp, 2)
        place = sp // 2
        x = lax.rem(place, xs)
        z = place // xs
        other = 1 - core
        head = 2 * y + core

        def at_z(step):
            return {"sp": (lax.rem(z + step + zs, zs) * xs + x) * 2 + core, "tp": y}

        def at_x(step):
            return {"sp": (z * xs + lax.rem(x + step + xs, xs)) * 2 + core, "tp": y}

        def at_y(step):
            return {"sp": sp, "tp": lax.rem(y + step + ys, ys)}

        def at_chip(step):
            chips = zs * xs
            return {"sp": lax.rem(place + step + chips, chips) * 2 + core, "tp": y}

        def at_partner():
            return {"sp": place * 2 + other, "tp": y}

        used, used_send = [0], [0]

        def recv_sem(count=1):
            k = used[0]
            used[0] += count
            return recv_sems.at[k]

        def send_sem():
            k = used_send[0]
            used_send[0] += 1
            return send_sems.at[k]

        def remote(src, dst, device, sem):
            return pltpu.make_async_remote_copy(
                src_ref=src, dst_ref=dst, send_sem=sem, recv_sem=recv_sem(),
                device_id=device, device_id_type=MESH,
            )

        def drain(sem, size):
            rows_sent = wbuf.reshape(zs * xs * 2 * rows, 512).at[pl.ds(0, size // 1024), :]
            pltpu.make_async_copy(rows_sent, rows_sent, sem).wait()

        rows = q1.shape[0]

        def by_head(h):
            a, b = h * 64, h * 64 + 64
            c, d = h * 128, h * 128 + 128
            return jnp.concatenate(
                [q1[:, a:b], q2[:, a:b], k1[:, a:b], k2[:, a:b], vw[:, c:d], pw[:, c:d]], axis=1
            )

        first, second = by_head(0), by_head(1)
        mine = core == 0
        own_rows = pl.ds(core * rows, rows)
        wbuf[z, x, own_rows, :] = jnp.where(mine, first, second)
        wsend[...] = jnp.where(mine, second, first)
        tokbuf[core, y] = tokens[...]
        wt[z, x, core] = jnp.concatenate(
            [oa[:, :128], op[:, :128], oa[:, 128:], op[:, 128:]], axis=1
        )
        qz[...] = jnp.zeros_like(qz)
        mbuf[...] = jnp.full(mbuf.shape, low_score, F32)
        lbuf[...] = jnp.zeros_like(lbuf)
        acc[...] = jnp.zeros_like(acc)

        barrier = pltpu.get_barrier_semaphore()
        neighbours = [
            at_z(1), at_z(-1), at_x(1), at_x(-1), at_y(1), at_y(-1), at_partner(), at_chip(1), at_chip(-1),
        ]
        for device in neighbours:
            pl.semaphore_signal(barrier, inc=1, device_id=device, device_id_type=MESH)
        pl.semaphore_wait(barrier, len(neighbours))

        misc_sem, share_sem, wt_share_sem, mean_sem, sum_sem = (send_sem() for _ in range(5))
        w_swap = remote(wsend, wbuf.at[z, x, own_rows, :], at_partner(), misc_sem)
        w_swap.start()
        half = tok // 2
        lead = rows
        rest = 2 * rows - lead
        row_bytes = 512 * 2
        lead_from, rest_from = core * rest, other * lead

        def pieces(first_row, size, p):
            return pl.ds(first_row, size) if p is None else pl.ds(first_row + p * (size // 2), size // 2)

        tok_ring = Ring(
            ys, y, at_y, lambda p, s: tokbuf.at[core, s, pl.ds(p * half, half), :],
            send_sem(), recv_sem,
        )
        lead_x = Ring(
            xs, x, at_x, lambda p, s: wbuf.at[z, s, pieces(lead_from, lead, p), :],
            send_sem(), recv_sem, True,
        )
        lead_z = Ring(
            zs, z, at_z, lambda p, s: wbuf.at[s, pl.ds(p * (xs // 2), xs // 2), pl.ds(lead_from, lead), :],
            send_sem(), recv_sem,
        )
        rest_z = Ring(
            zs, z, at_z, lambda p, s: wbuf.at[s, x, pieces(rest_from, rest, p), :],
            send_sem(), recv_sem, True,
        )
        wt_ring_z = Ring(
            zs, z, at_z, lambda p, s: wt.at[s, x, core, pieces(0, rows, p), :],
            send_sem(), recv_sem, True,
        )

        def half_z(p):
            return slice(None) if p is None else pl.ds(p * (zs // 2), zs // 2)

        wt_ring_x = Ring(
            xs, x, at_x, lambda p, s: wt.at[half_z(p), s, core], send_sem(), recv_sem, True
        )

        def rest_x_ring(slot):
            ring = Ring(
                xs, x, at_x, lambda p, s: wbuf.at[slot, s, pieces(rest_from, rest, p), :],
                send_sem(), recv_sem, True,
            )
            ring.begin()
            return ring

        lead_x.begin()
        tok_ring.begin()
        shared = []

        def share_tokens(s):
            copy = remote(tokbuf.at[core, s], tokbuf.at[core, s], at_partner(), share_sem)
            copy.start()
            shared.append(copy)

        share_tokens(y)
        cb, sb = cos_far[pl.ds(place, 1), :], sin_far[pl.ds(place, 1), :]
        w_swap.wait_recv()
        rest_z.begin()
        rest_x = [rest_x_ring(z)]

        def rest_step(h):
            if h <= zs // 2:
                rest_z.step(h)
                rest_x.append(rest_x_ring(rest_z.slot(0, h)))
                if h < zs // 2:
                    rest_x.append(rest_x_ring(rest_z.slot(1, h)))

        relayed = [0]

        def relay(count=zs):
            while relayed[0] < min(count, len(rest_x)):
                rest_x[relayed[0]].step(1)
                relayed[0] += 1

        def lead_step(h):
            if h <= zs // 2:
                lead_z.step(h)

        def tok_step(h):
            tok_ring.step(h)
            share_tokens(tok_ring.slot(0, h))
            if h < ys // 2:
                share_tokens(tok_ring.slot(1, h))

        wt_hops = list(range(1, zs // 2 + 1))

        def wt_next():
            if wt_hops:
                wt_ring_z.step(wt_hops.pop(0))

        lead_x.step(1)
        rest_step(1)
        lead_x.step(2)
        lead_z.begin()
        relay(1)
        rest_step(2)
        tok_step(1)
        rest_step(3)
        lead_step(1)
        relay(3)
        rest_step(4)
        lead_step(2)
        relay(5)
        tok_step(2)
        lead_step(3)
        relay(7)
        wt_ring_z.begin()
        for copy in shared:
            copy.wait_recv()

        for owner in range(2):
            square = jnp.zeros((tok, 1), F32)
            for s in range(ys):
                block = tokbuf[owner, s].astype(F32)
                square = square + jnp.sum(block * block, axis=1, keepdims=True)
            scale = lax.rsqrt(square * (1.0 / wide) + norm_floor)
            for s in range(ys):
                block = tokbuf[owner, s].astype(F32) * scale * gain[:, s * part : (s + 1) * part]
                nrm[owner * tok : (owner + 1) * tok, s * part : (s + 1) * part] = block.astype(BF16)

        lead_step(4)
        relay()
        for ring in rest_x:
            ring.step(2)
        wt_next()
        weight = wbuf[...].reshape(wide, 512)
        for cut in range(0, 512, 256):
            proj[:, cut : cut + 256] = dot(nrm[...], weight[:, cut : cut + 256])
        ca, sa = cos_near[...], sin_near[...]
        cosine = ca * cb - sa * sb
        sine = sa * cb + ca * sb
        low = lax.rem(lax.broadcasted_iota(jnp.int32, (chip, 128), 1), 64) < 32

        def turned(v):
            swapped = jnp.where(low, pltpu.roll(v, 96, 1), pltpu.roll(v, 32, 1))
            return v * cosine + swapped * sine

        pool = proj[:, 384:512].astype(BF16)
        pext[16 : 16 + chip, :] = pool.astype(F32)
        halo[0] = pool[chip - 16 :, :]
        to_next = remote(halo.at[0], halo.at[1], at_chip(1), send_sem())
        to_next.start()
        kbuf[z] = turned(proj[:, 128:256]).astype(BF16)
        vbuf[z] = proj[:, 256:384].T.astype(BF16)

        def kv_copy(d, h, u, slot):
            ref = kbuf.at[slot] if u == 0 else vbuf.at[slot]
            k = kv_first + (h - 1) * 4 + d * 2 + u
            return pltpu.make_async_remote_copy(
                src_ref=ref, dst_ref=ref, send_sem=kv_send, recv_sem=recv_sems.at[k],
                device_id=at_z(1 if d == 0 else -1), device_id_type=MESH,
            )

        kv_first = used[0]
        recv_sem(2 * zs)
        kv_send = send_sem()
        last = zs // 2

        def kv_slot(d, h):
            return lax.rem(z + (h if d else -h) + zs, zs)

        def kv_step(h):
            for u in (0, 1):
                for d in (0, 1):

                    @pl.when((h < last) | (d == u))
                    def _():
                        kv_copy(d, h, u, kv_slot(d, h)).wait_recv()

                        @pl.when((h + 1 < last) | ((h + 1 == last) & (d == u)))
                        def _():
                            kv_copy(d, h + 1, u, kv_slot(d, h)).start()

        for u in (0, 1):
            for d in (0, 1):
                if last > 1 or d == u:
                    kv_copy(d, 1, u, z).start()
        queries = (turned(proj[:, 0:128]) * (0.125 * math.log2(math.e))).T.astype(BF16)
        qz[x, 0:64, 0:chip] = queries[0:64]
        qz[x, 64:128, chip : 2 * chip] = queries[64:128]
        q_ring = Ring(
            xs, x, at_x,
            lambda p, s: qz.at[s, pl.ds(64 * p, 64), pl.ds(chip * p, chip)],
            send_sem(), recv_sem,
        )
        q_ring.begin()

        def attend(slot, chunks, masked=False):
            todo = [(ch, lt) for ch in chunks for lt in range(tiles)]

            def lanes_of(lt):
                return pl.ds(lt * LANE_TILE, LANE_TILE)

            def scores(ch, lt):
                return dot(kbuf[slot], qz[ch, :, lanes_of(lt)])

            def add_values(ch, lt, factor, p):
                lanes = lanes_of(lt)
                acc[ch, :, lanes] = acc[ch, :, lanes] * factor + dot(vbuf[slot], p)

            ready = [scores(*item) for item in todo[:2]]
            pending = None
            for k, (ch, lt) in enumerate(todo):
                if k + 2 < len(todo):
                    ready.append(scores(*todo[k + 2]))
                s = ready.pop(0)
                lanes = lanes_of(lt)
                if masked:
                    offset = (lt * LANE_TILE) % chip
                    visible = lax.broadcasted_iota(jnp.int32, s.shape, 0) <= (
                        lax.broadcasted_iota(jnp.int32, s.shape, 1) + offset
                    )
                    s = jnp.where(visible, s, low_score)
                before = mbuf[ch, 0:1, lanes]
                now = jnp.maximum(before, jnp.max(s, axis=0, keepdims=True))
                p = jnp.exp2(s - now)
                factor = jnp.exp2(before - now)
                mbuf[ch, 0:1, lanes] = now
                lbuf[ch, 0:1, lanes] = lbuf[ch, 0:1, lanes] * factor + jnp.sum(
                    p, axis=0, keepdims=True
                )
                if pending is not None:
                    add_values(*pending)
                pending = (ch, lt, factor, p.astype(BF16))
            add_values(*pending)

        attend(z, [x], True)
        wt_next()
        ahead = lax.rem(x + 1, xs)
        behind = lax.rem(x + xs - 1, xs)
        across = lax.rem(x + 2, xs)
        q_ring.step(1)
        wt_next()

        def own_block(k, carry):
            ch = jnp.where(k == 0, ahead, jnp.where(k == 1, behind, across))

            @pl.when(k == 2)
            def _():
                q_ring.step(2)

            @pl.when(ch > x)
            def _():
                attend(z, [ch])

            return carry

        lax.fori_loop(0, 3, own_block, 0)
        while wt_hops:
            wt_next()
        wt_ring_x.begin()
        to_next.wait_recv()
        prior = halo[1].astype(F32)
        pext[0:16, :] = jnp.where(place == 0, 0.0, prior)
        window = jnp.left_shift(2, lax.rem(head, 4))
        whole = pext[...]
        run = whole
        window_sum = jnp.zeros((chip, 128), F32)
        for k in range(4):
            lag = 1 << k
            run = run + jnp.concatenate(
                [jnp.zeros((lag, 128), F32), run[: 16 + chip - lag]], axis=0
            )
            window_sum = jnp.where(window == 2 * lag, run[16:], window_sum)
        position = place * chip + lax.broadcasted_iota(jnp.int32, (chip, 128), 0)
        count = jnp.minimum(position + 1, window).astype(F32)
        window_mean = (window_sum / count - whole[16:]).astype(BF16)
        pooled = (dot(window_mean, gw[head]) * pscale[pl.ds(head, 1), :]).astype(BF16)
        abuf[0, :, 128:256] = pooled[0:tok]
        abuf[1, :, 128:256] = pooled[tok:]
        wt_slots = [x, behind, ahead, across]
        wt_shared = [
            remote(wt.at[:, s, core], wt.at[:, s, core], at_partner(), wt_share_sem)
            for s in wt_slots
        ]

        wt_shared[0].start()

        def arrival(k, carry):
            h, d = k // 2 + 1, lax.rem(k, 2)

            @pl.when(d == 0)
            def _():
                kv_step(h)

            @pl.when(k == 4)
            def _():
                wt_ring_x.step(1)
                for copy in wt_shared[1:3]:
                    copy.start()

            slot = lax.rem(z + jnp.where(d == 0, -h, h) + zs, zs)

            @pl.when(slot < z)
            def _():
                attend(slot, [across, ahead, behind, x])

            return carry

        lax.fori_loop(0, zs - 2, arrival, 0)
        if zs == 2:
            wt_ring_x.step(1)
            for copy in wt_shared[1:3]:
                copy.start()
        kv_step(last)
        farthest = kv_slot(0, last)

        @pl.when(farthest < z)
        def _():
            attend(farthest, [across])

        def share(ch, m):
            lanes = pl.ds(m * chip, chip)
            total = lbuf[ch, 0:1, lanes]
            some = total > 0.0
            safe = jnp.where(some, total, 1.0)
            weight = jnp.where(some, mbuf[ch, 0:1, lanes] + jnp.log2(safe), low_score)
            return acc[ch, :, lanes] * (1.0 / safe), weight

        def put(pair, o_ref, e_ref):
            o_ref[...] = pair[0].astype(BF16)
            e_ref[...] = pair[1]

        def send_pair(o_src, e_src, o_dst, e_dst, device):
            pair = (remote(o_src, o_dst, device, mean_sem), remote(e_src, e_dst, device, send_sem()))
            for copy in pair:
                copy.start()
            stat_copies.append(pair[1])
            return pair

        stat_copies = []
        sides = ((ahead, at_x(1)), (behind, at_x(-1)))
        first_hop = []
        for m in (0, 1):
            put(share(across, m), o1s.at[m], e1s.at[m])
            first_hop.append(
                send_pair(o1s.at[m], e1s.at[m], o1r.at[m], e1r.at[m], sides[m][1])
            )

        @pl.when(farthest < z)
        def _():
            attend(farthest, [ahead, behind, x])

        wt_ring_x.step(2)
        wt_shared[3].start()
        def joined(*shares):
            top = shares[0][1]
            for _, weight in shares[1:]:
                top = jnp.maximum(top, weight)
            factors = [jnp.exp2(weight - top) for _, weight in shares]
            total = sum(factors)
            value = sum(o * f for (o, _), f in zip(shares, factors)) * (1.0 / total)
            return value, top + jnp.log2(total)

        def get(o_ref, e_ref):
            return o_ref[...].astype(F32), e_ref[...]

        second_hop = []
        for m in (0, 1):
            chunk, device = sides[m]
            k = 1 - m
            put(share(chunk, k), o2s.at[m, k], e2s.at[m, k])
            second_hop.append(
                send_pair(o2s.at[m, k], e2s.at[m, k], o2r.at[m, k], e2r.at[m, k], device)
            )
        for m in (0, 1):
            for copy in first_hop[m]:
                copy.wait_recv()
            chunk, device = sides[m]
            put(joined(share(chunk, m), get(o1r.at[m], e1r.at[m])), o2s.at[m, m], e2s.at[m, m])
            second_hop.append(
                send_pair(o2s.at[m, m], e2s.at[m, m], o2r.at[m, m], e2r.at[m, m], device)
            )
        for pair in second_hop:
            for copy in pair:
                copy.wait_recv()
        means = [
            joined(
                share(x, m),
                get(o2r.at[0, m], e2r.at[0, m]),
                get(o2r.at[1, m], e2r.at[1, m]),
            )[0]
            for m in (0, 1)
        ]
        difference = means[0] - lam[head] * means[1]
        norm = lax.rsqrt(jnp.mean(difference * difference, axis=0, keepdims=True) + head_floor)
        attn = ((difference * norm).T * hgain[...] * head_scale).astype(BF16)

        abuf[0, :, 0:128] = attn[0:tok]
        abuf[1, :, 0:128] = attn[tok:]
        swap = remote(abuf.at[other], abuf.at[2], at_partner(), send_sem())
        swap.start()
        swap.wait_recv()
        for copy in wt_shared:
            copy.wait_recv()

        rows_0 = jnp.where(core == 0, abuf[core], abuf[2])
        rows_1 = jnp.where(core == 0, abuf[2], abuf[core])
        per_z = wide // zs
        for s in range(zs):
            weight = wt[s].reshape(per_z, 512)
            ysum[:, s * per_z : (s + 1) * per_z] = (
                dot(rows_0, weight[:, 0:256], ((1,), (1,)))
                + dot(rows_1, weight[:, 256:512], ((1,), (1,)))
            ).astype(BF16)

        y_half = quarter // 2
        y_across = lax.rem(y + 2, ys)
        y_sides = (
            (lax.rem(y + 1, ys), at_y(1)),
            (lax.rem(y + ys - 1, ys), at_y(-1)),
        )

        def rows_of(target, m):
            return pl.ds(target * quarter + m * y_half, y_half)

        y_first, y_second = [], []

        def send_sum(src, dst, device, group):
            copy = remote(src, dst, device, sum_sem)
            copy.start()
            group.append(copy)

        for m in (0, 1):
            send_sum(ysum.at[rows_of(y_across, m), :], y1r.at[m], y_sides[m][1], y_first)
        for m in (0, 1):
            target, device = y_sides[m]
            send_sum(ysum.at[rows_of(target, 1 - m), :], y2r.at[m, 1 - m], device, y_second)
        for m in (0, 1):
            target, device = y_sides[m]
            y_first[m].wait_recv()
            y2s[m] = (
                ysum[rows_of(target, m), :].astype(F32) + y1r[m].astype(F32)
            ).astype(BF16)
            send_sum(y2s.at[m], y2r.at[m, m], device, y_second)
        for copy in y_second:
            copy.wait_recv()
        for m in (0, 1):
            out[m * y_half : (m + 1) * y_half, :] = (
                ysum[rows_of(y, m), :].astype(F32)
                + y2r[0, m].astype(F32)
                + y2r[1, m].astype(F32)
            ).astype(BF16)

        slot_bytes = (
            (tok_ring, tok * part * 2),
            (lead_x, lead * row_bytes),
            (lead_z, xs * lead * row_bytes),
            (rest_z, rest * row_bytes),
            *((ring, rest * row_bytes) for ring in rest_x),
            (wt_ring_z, rows * row_bytes),
            (wt_ring_x, zs * rows * row_bytes),
            (q_ring, chip * 256),
        )
        for ring, size in slot_bytes:
            drain(ring.send_sem, ring.sent_bytes(size))
        drain(kv_send, (zs - 1) * chip * 512)
        drain(share_sem, ys * tok * part * 2)
        drain(wt_share_sem, zs * xs * rows * row_bytes)
        drain(mean_sem, 6 * chip * 256)
        drain(sum_sem, 6 * (quarter // 2) * wide * 2)
        for copy in (w_swap, to_next, swap, *stat_copies):
            copy.wait_send()
        assert used[0] <= RECV_SEMAPHORES and used_send[0] <= SEND_SEMAPHORES, (used, used_send)

    return kernel


def solution(mesh):
    sp_size, ys = mesh.shape["sp"], mesh.shape["tp"]
    zs, xs = Z_SIZE, X_SIZE
    assert zs * xs * 2 == sp_size

    def body(
        tokens, norm_gain, query_one, key_one, query_two, key_two, value_weight, pool_weight,
        lambda_head, head_gain, group_weight, pool_scale, out_attn, out_pool,
    ):
        tok, part = tokens.shape
        wide = part * ys
        chip = 2 * tok
        rows = query_one.shape[0]
        quarter = tok // ys
        tables = rope_tables(chip, zs * xs)
        vmem = pl.BlockSpec(memory_space=pltpu.VMEM)
        smem = pl.BlockSpec(memory_space=pltpu.SMEM)
        args = (
            tokens, norm_gain.reshape(1, wide), query_one, key_one, query_two, key_two,
            value_weight, pool_weight, lambda_head, head_gain.reshape(1, 128), group_weight,
            pool_scale.reshape(-1, 128), out_attn.T, out_pool.T, *tables,
        )
        specs = [vmem] * len(args)
        specs[8] = smem
        return pl.pallas_call(
            make_kernel(zs, xs, ys, tok, wide),
            out_shape=jax.ShapeDtypeStruct((quarter, wide), BF16),
            in_specs=specs,
            out_specs=vmem,
            scratch_shapes=[
                pltpu.VMEM((rows, 512), BF16),
                pltpu.VMEM((zs, xs, 2 * rows, 512), BF16),
                pltpu.VMEM((zs, xs, 2, rows, 512), BF16),
                pltpu.VMEM((2, ys, tok, part), BF16),
                pltpu.VMEM((chip, wide), BF16),
                pltpu.VMEM((chip, 512), F32),
                pltpu.VMEM((zs, chip, 128), BF16),
                pltpu.VMEM((zs, 128, chip), BF16),
                pltpu.VMEM((xs, 128, 2 * chip), BF16),
                pltpu.VMEM((xs, 128, 2 * chip), F32),
                pltpu.VMEM((xs, 8, 2 * chip), F32),
                pltpu.VMEM((xs, 8, 2 * chip), F32),
                pltpu.VMEM((16 + chip, 128), F32),
                pltpu.VMEM((2, 16, 128), BF16),
                pltpu.VMEM((2, 128, chip), BF16),
                pltpu.VMEM((2, 1, chip), F32),
                pltpu.VMEM((2, 128, chip), BF16),
                pltpu.VMEM((2, 1, chip), F32),
                pltpu.VMEM((2, 2, 128, chip), BF16),
                pltpu.VMEM((2, 2, 1, chip), F32),
                pltpu.VMEM((2, 2, 128, chip), BF16),
                pltpu.VMEM((2, 2, 1, chip), F32),
                pltpu.VMEM((3, tok, 256), BF16),
                pltpu.VMEM((tok, wide), BF16),
                pltpu.VMEM((2, quarter // 2, wide), BF16),
                pltpu.VMEM((2, quarter // 2, wide), BF16),
                pltpu.VMEM((2, 2, quarter // 2, wide), BF16),
                pltpu.SemaphoreType.DMA((SEND_SEMAPHORES,)),
                pltpu.SemaphoreType.DMA((RECV_SEMAPHORES,)),
            ],
            compiler_params=pltpu.CompilerParams(
                collective_id=0, has_side_effects=True, vmem_limit_bytes=60 * 1024 * 1024
            ),
            name="mixer",
        )(*args)

    in_specs = (
        P("sp", "tp"),
        P(),
        P("sp", "tp"),
        P("sp", "tp"),
        P("sp", "tp"),
        P("sp", "tp"),
        P("sp", "tp"),
        P("sp", "tp"),
        P(),
        P(),
        P(),
        P(),
        P("tp", "sp"),
        P("tp", "sp"),
    )
    out_specs = P(("sp", "tp"), None)
    return jax.shard_map(body, mesh=mesh, in_specs=in_specs, out_specs=out_specs, check_vma=False)
```

```python
import math

import jax
import jax.numpy as jnp
import numpy as np
from jax import lax
from jax.experimental import pallas as pl
from jax.experimental.pallas import tpu as pltpu
from jax.sharding import PartitionSpec as P

MESH = pl.DeviceIdType.MESH
F32 = jnp.float32
BF16 = jnp.bfloat16
Z_SIZE = 8
X_SIZE = 4
LANE_TILE = 256
SEND_SEMAPHORES = 32
RECV_SEMAPHORES = 128

rope_base = 500000.0
head_scale = 0.8
norm_floor = 1e-06
head_floor = 0.001
low_score = -1e30


def rope_tables(chip_tokens, chips):
    lane = np.arange(128)
    inverse = rope_base ** (-((lane % 32) * 2.0 / 64.0))
    sign = np.where(lane % 64 < 32, -1.0, 1.0)
    near = np.arange(chip_tokens)[:, None] * inverse[None, :]
    far = (np.arange(chips) * chip_tokens)[:, None] * inverse[None, :]
    return (
        np.cos(near).astype(np.float32),
        (np.sin(near) * sign).astype(np.float32),
        np.cos(far).astype(np.float32),
        (np.sin(far) * sign).astype(np.float32),
    )


class Ring:
    def __init__(self, n, me, device, unit, send_sem, recv_sem, whole=False):
        self.n, self.me, self.device, self.unit, self.whole = n, me, device, unit, whole
        self.send_sem = send_sem
        self.recv = {(d, h, p): recv_sem() for h in range(1, n // 2 + 1) for d in (0, 1) for p in self.parts(d, h)}

    def parts(self, d, h):
        if h == self.n // 2:
            return (d,)
        return (None,) if self.whole else (0, 1)

    def slot(self, d, h):
        return lax.rem(self.me + (h if d else -h) + self.n, self.n)

    def copy(self, d, h, p, slot):
        ref = self.unit(p, slot)
        return pltpu.make_async_remote_copy(
            src_ref=ref,
            dst_ref=ref,
            send_sem=self.send_sem,
            recv_sem=self.recv[d, h, p],
            device_id=self.device(-1 if d else 1),
            device_id_type=MESH,
        )

    def send(self, d, h, p):
        self.copy(d, h, p, self.slot(d, h - 1)).start()

    def begin(self):
        for d in (0, 1):
            for p in self.parts(d, 1):
                self.send(d, 1, p)

    def step(self, h):
        units = (None,) if self.whole else (0, 1)
        for p in units if h < self.n // 2 else (0, 1):
            for d in (0, 1):
                if p in self.parts(d, h):
                    self.copy(d, h, p, self.slot(d, h)).wait_recv()
                    if h + 1 < self.n // 2:
                        self.send(d, h + 1, p)
                    elif h + 1 == self.n // 2 and p in (None, d):
                        self.send(d, h + 1, d)

    def sent_bytes(self, slot_bytes):
        return sum(slot_bytes if p is None else slot_bytes // 2 for _, _, p in self.recv)


def dot(a, b, dims=((1,), (0,))):
    return lax.dot_general(a, b, (dims, ((), ())), preferred_element_type=F32)


def make_kernel(zs, xs, ys, tok, wide):
    chip = 2 * tok
    part = wide // ys
    quarter = tok // ys
    tiles = 2 * chip // LANE_TILE

    def kernel(
        tokens, gain, q1, k1, q2, k2, vw, pw, lam, hgain, gw, pscale, oa, op,
        cos_near, sin_near, cos_far, sin_far,
        out,
        wsend, wbuf, wt, tokbuf, nrm, proj, kbuf, vbuf, qz, acc, mbuf, lbuf,
        pext, halo, o1s, e1s, o1r, e1r, o2s, e2s, o2r, e2r, abuf,
        ysum, y1r, y2s, y2r, send_sems, recv_sems,
    ):
        sp = lax.axis_index("sp")
        y = lax.axis_index("tp")
        core = lax.rem(sp, 2)
        place = sp // 2
        x = lax.rem(place, xs)
        z = place // xs
        other = 1 - core
        head = 2 * y + core

        def at_z(step):
            return {"sp": (lax.rem(z + step + zs, zs) * xs + x) * 2 + core, "tp": y}

        def at_x(step):
            return {"sp": (z * xs + lax.rem(x + step + xs, xs)) * 2 + core, "tp": y}

        def at_y(step):
            return {"sp": sp, "tp": lax.rem(y + step + ys, ys)}

        def at_chip(step):
            chips = zs * xs
            return {"sp": lax.rem(place + step + chips, chips) * 2 + core, "tp": y}

        def at_partner():
            return {"sp": place * 2 + other, "tp": y}

        used, used_send = [0], [0]

        def recv_sem(count=1):
            k = used[0]
            used[0] += count
            return recv_sems.at[k]

        def send_sem():
            k = used_send[0]
            used_send[0] += 1
            return send_sems.at[k]

        def remote(src, dst, device, sem):
            return pltpu.make_async_remote_copy(
                src_ref=src, dst_ref=dst, send_sem=sem, recv_sem=recv_sem(),
                device_id=device, device_id_type=MESH,
            )

        def drain(sem, size):
            rows_sent = wbuf.reshape(zs * xs * 2 * rows, 512).at[pl.ds(0, size // 1024), :]
            pltpu.make_async_copy(rows_sent, rows_sent, sem).wait()

        rows = q1.shape[0]

        def by_head(h):
            a, b = h * 64, h * 64 + 64
            c, d = h * 128, h * 128 + 128
            return jnp.concatenate(
                [q1[:, a:b], q2[:, a:b], k1[:, a:b], k2[:, a:b], vw[:, c:d], pw[:, c:d]], axis=1
            )

        first, second = by_head(0), by_head(1)
        mine = core == 0
        own_rows = pl.ds(core * rows, rows)
        wbuf[z, x, own_rows, :] = jnp.where(mine, first, second)
        wsend[...] = jnp.where(mine, second, first)
        tokbuf[core, y] = tokens[...]
        wt[z, x, core] = jnp.concatenate(
            [oa[:, :128], op[:, :128], oa[:, 128:], op[:, 128:]], axis=1
        )
        qz[...] = jnp.zeros_like(qz)
        mbuf[...] = jnp.full(mbuf.shape, low_score, F32)
        lbuf[...] = jnp.zeros_like(lbuf)
        acc[...] = jnp.zeros_like(acc)

        barrier = pltpu.get_barrier_semaphore()
        neighbours = [
            at_z(1), at_z(-1), at_x(1), at_x(-1), at_y(1), at_y(-1), at_partner(), at_chip(1), at_chip(-1),
        ]
        for device in neighbours:
            pl.semaphore_signal(barrier, inc=1, device_id=device, device_id_type=MESH)
        pl.semaphore_wait(barrier, len(neighbours))

        misc_sem, share_sem, wt_share_sem, mean_sem, sum_sem = (send_sem() for _ in range(5))
        w_swap = remote(wsend, wbuf.at[z, x, own_rows, :], at_partner(), misc_sem)
        w_swap.start()
        half = tok // 2
        lead = rows
        rest = 2 * rows - lead
        row_bytes = 512 * 2
        lead_from, rest_from = core * rest, other * lead

        def pieces(first_row, size, p):
            return pl.ds(first_row, size) if p is None else pl.ds(first_row + p * (size // 2), size // 2)

        tok_ring = Ring(
            ys, y, at_y, lambda p, s: tokbuf.at[core, s, pl.ds(p * half, half), :],
            send_sem(), recv_sem,
        )
        lead_x = Ring(
            xs, x, at_x, lambda p, s: wbuf.at[z, s, pieces(lead_from, lead, p), :],
            send_sem(), recv_sem, True,
        )
        lead_z = Ring(
            zs, z, at_z, lambda p, s: wbuf.at[s, pl.ds(p * (xs // 2), xs // 2), pl.ds(lead_from, lead), :],
            send_sem(), recv_sem,
        )
        rest_z = Ring(
            zs, z, at_z, lambda p, s: wbuf.at[s, x, pieces(rest_from, rest, p), :],
            send_sem(), recv_sem, True,
        )
        wt_ring_z = Ring(
            zs, z, at_z, lambda p, s: wt.at[s, x, core, pieces(0, rows, p), :],
            send_sem(), recv_sem, True,
        )

        def half_z(p):
            return slice(None) if p is None else pl.ds(p * (zs // 2), zs // 2)

        wt_ring_x = Ring(
            xs, x, at_x, lambda p, s: wt.at[half_z(p), s, core], send_sem(), recv_sem, True
        )

        def rest_x_ring(slot):
            ring = Ring(
                xs, x, at_x, lambda p, s: wbuf.at[slot, s, pieces(rest_from, rest, p), :],
                send_sem(), recv_sem, True,
            )
            ring.begin()
            return ring

        lead_x.begin()
        tok_ring.begin()
        shared = []

        def share_tokens(s):
            copy = remote(tokbuf.at[core, s], tokbuf.at[core, s], at_partner(), share_sem)
            copy.start()
            shared.append(copy)

        share_tokens(y)
        cb, sb = cos_far[pl.ds(place, 1), :], sin_far[pl.ds(place, 1), :]
        w_swap.wait_recv()
        rest_z.begin()
        rest_x = [rest_x_ring(z)]

        def rest_step(h):
            if h <= zs // 2:
                rest_z.step(h)
                rest_x.append(rest_x_ring(rest_z.slot(0, h)))
                if h < zs // 2:
                    rest_x.append(rest_x_ring(rest_z.slot(1, h)))

        relayed = [0]

        def relay(count=zs):
            while relayed[0] < min(count, len(rest_x)):
                rest_x[relayed[0]].step(1)
                relayed[0] += 1

        def lead_step(h):
            if h <= zs // 2:
                lead_z.step(h)

        def tok_step(h):
            tok_ring.step(h)
            share_tokens(tok_ring.slot(0, h))
            if h < ys // 2:
                share_tokens(tok_ring.slot(1, h))

        wt_hops = list(range(1, zs // 2 + 1))

        def wt_next():
            if wt_hops:
                wt_ring_z.step(wt_hops.pop(0))

        lead_x.step(1)
        rest_step(1)
        lead_x.step(2)
        lead_z.begin()
        wt_ring_z.begin()
        relay(1)
        rest_step(2)
        tok_step(1)
        relay(3)
        wt_next()
        lead_step(1)
        rest_step(3)
        wt_next()
        rest_step(4)
        relay(5)
        lead_step(2)
        relay(7)
        wt_next()
        tok_step(2)
        relay(8)
        lead_step(3)
        for copy in shared:
            copy.wait_recv()

        for owner in range(2):
            square = jnp.zeros((tok, 1), F32)
            for s in range(ys):
                block = tokbuf[owner, s].astype(F32)
                square = square + jnp.sum(block * block, axis=1, keepdims=True)
            scale = lax.rsqrt(square * (1.0 / wide) + norm_floor)
            for s in range(ys):
                block = tokbuf[owner, s].astype(F32) * scale * gain[:, s * part : (s + 1) * part]
                nrm[owner * tok : (owner + 1) * tok, s * part : (s + 1) * part] = block.astype(BF16)

        lead_step(4)
        for ring in rest_x:
            ring.step(2)
        wt_next()
        weight = wbuf[...].reshape(wide, 512)
        for cut in range(0, 512, 256):
            proj[:, cut : cut + 256] = dot(nrm[...], weight[:, cut : cut + 256])
        ca, sa = cos_near[...], sin_near[...]
        cosine = ca * cb - sa * sb
        sine = sa * cb + ca * sb
        low = lax.rem(lax.broadcasted_iota(jnp.int32, (chip, 128), 1), 64) < 32

        def turned(v):
            swapped = jnp.where(low, pltpu.roll(v, 96, 1), pltpu.roll(v, 32, 1))
            return v * cosine + swapped * sine

        pool = proj[:, 384:512].astype(BF16)
        pext[16 : 16 + chip, :] = pool.astype(F32)
        halo[0] = pool[chip - 16 :, :]
        to_next = remote(halo.at[0], halo.at[1], at_chip(1), send_sem())
        to_next.start()
        kbuf[z] = turned(proj[:, 128:256]).astype(BF16)
        vbuf[z] = proj[:, 256:384].T.astype(BF16)

        def kv_copy(d, h, u, slot):
            ref = kbuf.at[slot] if u == 0 else vbuf.at[slot]
            k = kv_first + (h - 1) * 4 + d * 2 + u
            return pltpu.make_async_remote_copy(
                src_ref=ref, dst_ref=ref, send_sem=kv_send, recv_sem=recv_sems.at[k],
                device_id=at_z(1 if d == 0 else -1), device_id_type=MESH,
            )

        kv_first = used[0]
        recv_sem(2 * zs)
        kv_send = send_sem()
        last = zs // 2

        def kv_slot(d, h):
            return lax.rem(z + (h if d else -h) + zs, zs)

        def kv_step(h):
            for u in (0, 1):
                for d in (0, 1):

                    @pl.when((h < last) | (d == u))
                    def _():
                        kv_copy(d, h, u, kv_slot(d, h)).wait_recv()

                        @pl.when((h + 1 < last) | ((h + 1 == last) & (d == u)))
                        def _():
                            kv_copy(d, h + 1, u, kv_slot(d, h)).start()

        for u in (0, 1):
            for d in (0, 1):
                if last > 1 or d == u:
                    kv_copy(d, 1, u, z).start()
        queries = (turned(proj[:, 0:128]) * (0.125 * math.log2(math.e))).T.astype(BF16)
        qz[x, 0:64, 0:chip] = queries[0:64]
        qz[x, 64:128, chip : 2 * chip] = queries[64:128]
        q_ring = Ring(
            xs, x, at_x,
            lambda p, s: qz.at[s, pl.ds(64 * p, 64), pl.ds(chip * p, chip)],
            send_sem(), recv_sem,
        )
        q_ring.begin()

        def attend(slot, chunks, masked=False):
            todo = [(ch, lt) for ch in chunks for lt in range(tiles)]

            def lanes_of(lt):
                return pl.ds(lt * LANE_TILE, LANE_TILE)

            def scores(ch, lt):
                return dot(kbuf[slot], qz[ch, :, lanes_of(lt)])

            def add_values(ch, lt, factor, p):
                lanes = lanes_of(lt)
                acc[ch, :, lanes] = acc[ch, :, lanes] * factor + dot(vbuf[slot], p)

            ready = [scores(*item) for item in todo[:2]]
            pending = None
            for k, (ch, lt) in enumerate(todo):
                if k + 2 < len(todo):
                    ready.append(scores(*todo[k + 2]))
                s = ready.pop(0)
                lanes = lanes_of(lt)
                if masked:
                    offset = (lt * LANE_TILE) % chip
                    visible = lax.broadcasted_iota(jnp.int32, s.shape, 0) <= (
                        lax.broadcasted_iota(jnp.int32, s.shape, 1) + offset
                    )
                    s = jnp.where(visible, s, low_score)
                before = mbuf[ch, 0:1, lanes]
                now = jnp.maximum(before, jnp.max(s, axis=0, keepdims=True))
                p = jnp.exp2(s - now)
                factor = jnp.exp2(before - now)
                mbuf[ch, 0:1, lanes] = now
                lbuf[ch, 0:1, lanes] = lbuf[ch, 0:1, lanes] * factor + jnp.sum(
                    p, axis=0, keepdims=True
                )
                if pending is not None:
                    add_values(*pending)
                pending = (ch, lt, factor, p.astype(BF16))
            add_values(*pending)

        attend(z, [x], True)
        ahead = lax.rem(x + 1, xs)
        behind = lax.rem(x + xs - 1, xs)
        across = lax.rem(x + 2, xs)
        q_ring.step(1)

        def own_block(k, carry):
            ch = jnp.where(k == 0, ahead, jnp.where(k == 1, behind, across))

            @pl.when(k == 2)
            def _():
                q_ring.step(2)

            @pl.when(ch > x)
            def _():
                attend(z, [ch])

            return carry

        lax.fori_loop(0, 3, own_block, 0)
        wt_ring_x.begin()
        to_next.wait_recv()
        prior = halo[1].astype(F32)
        pext[0:16, :] = jnp.where(place == 0, 0.0, prior)
        window = jnp.left_shift(2, lax.rem(head, 4))
        whole = pext[...]
        run = whole
        window_sum = jnp.zeros((chip, 128), F32)
        for k in range(4):
            lag = 1 << k
            run = run + jnp.concatenate(
                [jnp.zeros((lag, 128), F32), run[: 16 + chip - lag]], axis=0
            )
            window_sum = jnp.where(window == 2 * lag, run[16:], window_sum)
        position = place * chip + lax.broadcasted_iota(jnp.int32, (chip, 128), 0)
        count = jnp.minimum(position + 1, window).astype(F32)
        window_mean = (window_sum / count - whole[16:]).astype(BF16)
        pooled = (dot(window_mean, gw[head]) * pscale[pl.ds(head, 1), :]).astype(BF16)
        abuf[0, :, 128:256] = pooled[0:tok]
        abuf[1, :, 128:256] = pooled[tok:]
        wt_slots = [x, behind, ahead, across]
        wt_shared = [
            remote(wt.at[:, s, core], wt.at[:, s, core], at_partner(), wt_share_sem)
            for s in wt_slots
        ]

        wt_shared[0].start()

        def arrival(k, carry):
            h, d = k // 2 + 1, lax.rem(k, 2)

            @pl.when(d == 0)
            def _():
                kv_step(h)

            @pl.when(k == 4)
            def _():
                wt_ring_x.step(1)
                for copy in wt_shared[1:3]:
                    copy.start()

            slot = lax.rem(z + jnp.where(d == 0, -h, h) + zs, zs)

            @pl.when(slot < z)
            def _():
                attend(slot, [across, ahead, behind, x])

            return carry

        lax.fori_loop(0, zs - 2, arrival, 0)
        if zs == 2:
            wt_ring_x.step(1)
            for copy in wt_shared[1:3]:
                copy.start()
        kv_step(last)
        farthest = kv_slot(0, last)

        @pl.when(farthest < z)
        def _():
            attend(farthest, [across])

        def share(ch, m):
            lanes = pl.ds(m * chip, chip)
            total = lbuf[ch, 0:1, lanes]
            some = total > 0.0
            safe = jnp.where(some, total, 1.0)
            weight = jnp.where(some, mbuf[ch, 0:1, lanes] + jnp.log2(safe), low_score)
            return acc[ch, :, lanes] * (1.0 / safe), weight

        def put(pair, o_ref, e_ref):
            o_ref[...] = pair[0].astype(BF16)
            e_ref[...] = pair[1]

        def send_pair(o_src, e_src, o_dst, e_dst, device):
            pair = (remote(o_src, o_dst, device, mean_sem), remote(e_src, e_dst, device, send_sem()))
            for copy in pair:
                copy.start()
            stat_copies.append(pair[1])
            return pair

        stat_copies = []
        sides = ((ahead, at_x(1)), (behind, at_x(-1)))
        first_hop = []
        for m in (0, 1):
            put(share(across, m), o1s.at[m], e1s.at[m])
            first_hop.append(
                send_pair(o1s.at[m], e1s.at[m], o1r.at[m], e1r.at[m], sides[m][1])
            )

        @pl.when(farthest < z)
        def _():
            attend(farthest, [ahead, behind, x])

        wt_ring_x.step(2)
        wt_shared[3].start()
        def joined(*shares):
            top = shares[0][1]
            for _, weight in shares[1:]:
                top = jnp.maximum(top, weight)
            factors = [jnp.exp2(weight - top) for _, weight in shares]
            total = sum(factors)
            value = sum(o * f for (o, _), f in zip(shares, factors)) * (1.0 / total)
            return value, top + jnp.log2(total)

        def get(o_ref, e_ref):
            return o_ref[...].astype(F32), e_ref[...]

        second_hop = []
        for m in (0, 1):
            chunk, device = sides[m]
            k = 1 - m
            put(share(chunk, k), o2s.at[m, k], e2s.at[m, k])
            second_hop.append(
                send_pair(o2s.at[m, k], e2s.at[m, k], o2r.at[m, k], e2r.at[m, k], device)
            )
        for m in (0, 1):
            for copy in first_hop[m]:
                copy.wait_recv()
            chunk, device = sides[m]
            put(joined(share(chunk, m), get(o1r.at[m], e1r.at[m])), o2s.at[m, m], e2s.at[m, m])
            second_hop.append(
                send_pair(o2s.at[m, m], e2s.at[m, m], o2r.at[m, m], e2r.at[m, m], device)
            )
        for pair in second_hop:
            for copy in pair:
                copy.wait_recv()
        means = [
            joined(
                share(x, m),
                get(o2r.at[0, m], e2r.at[0, m]),
                get(o2r.at[1, m], e2r.at[1, m]),
            )[0]
            for m in (0, 1)
        ]
        difference = means[0] - lam[head] * means[1]
        norm = lax.rsqrt(jnp.mean(difference * difference, axis=0, keepdims=True) + head_floor)
        attn = ((difference * norm).T * hgain[...] * head_scale).astype(BF16)

        abuf[0, :, 0:128] = attn[0:tok]
        abuf[1, :, 0:128] = attn[tok:]
        swap = remote(abuf.at[other], abuf.at[2], at_partner(), send_sem())
        swap.start()
        swap.wait_recv()
        for copy in wt_shared:
            copy.wait_recv()

        rows_0 = jnp.where(core == 0, abuf[core], abuf[2])
        rows_1 = jnp.where(core == 0, abuf[2], abuf[core])
        per_z = wide // zs
        for s in range(zs):
            weight = wt[s].reshape(per_z, 512)
            ysum[:, s * per_z : (s + 1) * per_z] = (
                dot(rows_0, weight[:, 0:256], ((1,), (1,)))
                + dot(rows_1, weight[:, 256:512], ((1,), (1,)))
            ).astype(BF16)

        y_half = quarter // 2
        y_across = lax.rem(y + 2, ys)
        y_sides = (
            (lax.rem(y + 1, ys), at_y(1)),
            (lax.rem(y + ys - 1, ys), at_y(-1)),
        )

        def rows_of(target, m):
            return pl.ds(target * quarter + m * y_half, y_half)

        y_first, y_second = [], []

        def send_sum(src, dst, device, group):
            copy = remote(src, dst, device, sum_sem)
            copy.start()
            group.append(copy)

        for m in (0, 1):
            send_sum(ysum.at[rows_of(y_across, m), :], y1r.at[m], y_sides[m][1], y_first)
        for m in (0, 1):
            target, device = y_sides[m]
            send_sum(ysum.at[rows_of(target, 1 - m), :], y2r.at[m, 1 - m], device, y_second)
        for m in (0, 1):
            target, device = y_sides[m]
            y_first[m].wait_recv()
            y2s[m] = (
                ysum[rows_of(target, m), :].astype(F32) + y1r[m].astype(F32)
            ).astype(BF16)
            send_sum(y2s.at[m], y2r.at[m, m], device, y_second)
        for copy in y_second:
            copy.wait_recv()
        for m in (0, 1):
            out[m * y_half : (m + 1) * y_half, :] = (
                ysum[rows_of(y, m), :].astype(F32)
                + y2r[0, m].astype(F32)
                + y2r[1, m].astype(F32)
            ).astype(BF16)

        slot_bytes = (
            (tok_ring, tok * part * 2),
            (lead_x, lead * row_bytes),
            (lead_z, xs * lead * row_bytes),
            (rest_z, rest * row_bytes),
            *((ring, rest * row_bytes) for ring in rest_x),
            (wt_ring_z, rows * row_bytes),
            (wt_ring_x, zs * rows * row_bytes),
            (q_ring, chip * 256),
        )
        for ring, size in slot_bytes:
            drain(ring.send_sem, ring.sent_bytes(size))
        drain(kv_send, (zs - 1) * chip * 512)
        drain(share_sem, ys * tok * part * 2)
        drain(wt_share_sem, zs * xs * rows * row_bytes)
        drain(mean_sem, 6 * chip * 256)
        drain(sum_sem, 6 * (quarter // 2) * wide * 2)
        for copy in (w_swap, to_next, swap, *stat_copies):
            copy.wait_send()
        assert used[0] <= RECV_SEMAPHORES and used_send[0] <= SEND_SEMAPHORES, (used, used_send)

    return kernel


def solution(mesh):
    sp_size, ys = mesh.shape["sp"], mesh.shape["tp"]
    zs, xs = Z_SIZE, X_SIZE
    assert zs * xs * 2 == sp_size

    def body(
        tokens, norm_gain, query_one, key_one, query_two, key_two, value_weight, pool_weight,
        lambda_head, head_gain, group_weight, pool_scale, out_attn, out_pool,
    ):
        tok, part = tokens.shape
        wide = part * ys
        chip = 2 * tok
        rows = query_one.shape[0]
        quarter = tok // ys
        tables = rope_tables(chip, zs * xs)
        vmem = pl.BlockSpec(memory_space=pltpu.VMEM)
        smem = pl.BlockSpec(memory_space=pltpu.SMEM)
        args = (
            tokens, norm_gain.reshape(1, wide), query_one, key_one, query_two, key_two,
            value_weight, pool_weight, lambda_head, head_gain.reshape(1, 128), group_weight,
            pool_scale.reshape(-1, 128), out_attn.T, out_pool.T, *tables,
        )
        specs = [vmem] * len(args)
        specs[8] = smem
        return pl.pallas_call(
            make_kernel(zs, xs, ys, tok, wide),
            out_shape=jax.ShapeDtypeStruct((quarter, wide), BF16),
            in_specs=specs,
            out_specs=vmem,
            scratch_shapes=[
                pltpu.VMEM((rows, 512), BF16),
                pltpu.VMEM((zs, xs, 2 * rows, 512), BF16),
                pltpu.VMEM((zs, xs, 2, rows, 512), BF16),
                pltpu.VMEM((2, ys, tok, part), BF16),
                pltpu.VMEM((chip, wide), BF16),
                pltpu.VMEM((chip, 512), F32),
                pltpu.VMEM((zs, chip, 128), BF16),
                pltpu.VMEM((zs, 128, chip), BF16),
                pltpu.VMEM((xs, 128, 2 * chip), BF16),
                pltpu.VMEM((xs, 128, 2 * chip), F32),
                pltpu.VMEM((xs, 8, 2 * chip), F32),
                pltpu.VMEM((xs, 8, 2 * chip), F32),
                pltpu.VMEM((16 + chip, 128), F32),
                pltpu.VMEM((2, 16, 128), BF16),
                pltpu.VMEM((2, 128, chip), BF16),
                pltpu.VMEM((2, 1, chip), F32),
                pltpu.VMEM((2, 128, chip), BF16),
                pltpu.VMEM((2, 1, chip), F32),
                pltpu.VMEM((2, 2, 128, chip), BF16),
                pltpu.VMEM((2, 2, 1, chip), F32),
                pltpu.VMEM((2, 2, 128, chip), BF16),
                pltpu.VMEM((2, 2, 1, chip), F32),
                pltpu.VMEM((3, tok, 256), BF16),
                pltpu.VMEM((tok, wide), BF16),
                pltpu.VMEM((2, quarter // 2, wide), BF16),
                pltpu.VMEM((2, quarter // 2, wide), BF16),
                pltpu.VMEM((2, 2, quarter // 2, wide), BF16),
                pltpu.SemaphoreType.DMA((SEND_SEMAPHORES,)),
                pltpu.SemaphoreType.DMA((RECV_SEMAPHORES,)),
            ],
            compiler_params=pltpu.CompilerParams(
                collective_id=0, has_side_effects=True, vmem_limit_bytes=60 * 1024 * 1024
            ),
            name="mixer",
        )(*args)

    in_specs = (
        P("sp", "tp"),
        P(),
        P("sp", "tp"),
        P("sp", "tp"),
        P("sp", "tp"),
        P("sp", "tp"),
        P("sp", "tp"),
        P("sp", "tp"),
        P(),
        P(),
        P(),
        P(),
        P("tp", "sp"),
        P("tp", "sp"),
    )
    out_specs = P(("sp", "tp"), None)
    return jax.shard_map(body, mesh=mesh, in_specs=in_specs, out_specs=out_specs, check_vma=False)
```
